512 devices in a mesh: ep: 32 (over z, core), tp: 16 (over y, x).
Axes of the slice: x: 4, y: 4, z: 16, core: 2. Of those that a mesh axis runs over, the one named last changes fastest.
Arguments:
- attn_in: bfloat16 [16384, 2048], P('ep'), may hold values from -6 to 6
- mix_gain: float32 [2048], replicated, may hold values from 0.1 to 1.9
- query_weight: bfloat16 [2048, 1024], P(None, 'tp'), may hold values from -0.125 to 0.125
- key_weight: bfloat16 [2048, 1024], P(None, 'tp'), may hold values from -0.125 to 0.125
- value_weight: bfloat16 [2048, 1024], P(None, 'tp'), may hold values from -0.125 to 0.125
- query_gain: float32 [64], replicated, may hold values from 0.7 to 6
- key_gain: float32 [64], replicated, may hold values from 0.7 to 6
- log_cache: float32 [16384, 16], P('ep', 'tp'), as said below
- head_gain: float32 [1024], P('tp'), may hold values from 0.1 to 1.9
- out_weight: bfloat16 [1024, 2048], P(None, 'tp'), may hold values from -0.1875 to 0.1875
- moe_in: bfloat16 [4096, 2048], P('ep'), may hold values from -6 to 6
- moe_gain: float32 [2048], replicated, may hold values from 0.1 to 1.9
- routes: int32 [4096, 2], P('ep'), may hold values from 0 to 31, all different within a row; in each aligned block of 128 rows (0 to 127, 128 to 255, ...) at most 12 rows name the same one
- route_weight: float32 [4096, 2], P('ep'), may hold values from 0.25 to 1
- expert_gate: bfloat16 [32, 2048, 1024], P('ep', None, 'tp'), may hold values from -0.125 to 0.125
- expert_up: bfloat16 [32, 2048, 1024], P('ep', None, 'tp'), may hold values from -0.125 to 0.125
- expert_down: bfloat16 [32, 1024, 2048], P('ep', 'tp'), may hold values from -0.1875 to 0.1875
Outputs:
- mixer_out: bfloat16 [16384, 2048], P('ep', 'tp')
- moe_out: bfloat16 [4096, 2048], P('ep', 'tp')
The draws below stay inside these ranges and needn't reach their ends.
Inputs may be any that keep to these rules, and one draw needn't show every extreme that they name: `routes`: each row names 2 different experts; within the rows of one index of ep (aligned blocks of 128 rows) no expert is named by more than 12 rows. `log_cache`: never increasing along positions for each head.
All inputs are finite; a program needn't handle non-finite values.
Results may differ from the reference program's by a relative error of at most 0.015.
The reference program's roundings to bfloat16 on the way count: a program that leaves them out, or rounds other values in their place, can miss the bound.
Values may be sent and summed in bfloat16 or wider, within the bound.
A program may use at most 64 MiB of HBM per device.

```python
import math
import jax
import jax.numpy as jnp
import numpy as np
from jax import lax

D = 2048
HEADS = 16
HD = 64
FFE = 1024
TOPK = 2
TOK_DEV = 512
TOK_MOE = 128
TOKENS = 16384
TOKENS2 = 4096
EXPERTS = 32
CAP = 12
N_EP = 32


def draw_log_cache(key, part):
    first_key = jax.random.fold_in(key, 31)
    second_key = jax.random.fold_in(key, 32)
    third_key = jax.random.fold_in(key, 33)
    fast_heads = jax.random.uniform(first_key, (HEADS,), jnp.float32) < 0.5
    base_rate = jnp.where(fast_heads, 1.0 / 40.0, 1.5 / TOKENS)
    block_count = TOKENS // TOK_DEV
    block_factor = jnp.exp(jax.random.uniform(second_key, (block_count, 1, HEADS), jnp.float32, -0.7, 0.7))
    block_factor = jnp.broadcast_to(block_factor, (block_count, TOK_DEV, HEADS)).reshape(TOKENS, HEADS)
    rough_factor = jax.random.uniform(third_key, (TOKENS, HEADS), jnp.float32, 0.3, 1.7)
    return -jnp.cumsum(base_rate[None, :] * block_factor * rough_factor, axis=0)


def draw_query_gain(key, part):
    gain_key = jax.random.fold_in(key, 11)
    return jax.random.uniform(gain_key, (HD,), jnp.float32, 0.7, 1.3)


def draw_key_gain(key, part):
    gain_key = jax.random.fold_in(key, 12)
    return jax.random.uniform(gain_key, (HD,), jnp.float32, 0.7, 1.3)


def shard_levels(own_key, extent, pieces, smallest, top_value):
    loudness = 1.0
    for position, blocks in pieces:
        heights = jax.random.uniform(jax.random.fold_in(jax.random.fold_in(own_key, 6), position), (blocks,), jnp.float32, smallest / len(pieces), top_value / len(pieces))
        loudness = loudness * jnp.repeat(jnp.exp(heights), extent[position] // blocks).reshape((-1,) + (1,) * (len(extent) - 1 - position))
    return loudness


def assign_block(stream_key, own, number, rows, number_of, top, reach, slope):
    sequence = jax.random.permutation(stream_key, number_of)
    packed, usual = load_shares(number_of, rows * top, reach, slope, True), load_shares(number_of, rows * top, reach, slope, False)
    places = jnp.arange(number_of)

    def named(sizes, rotation):
        used = int((sizes > 0).sum())
        fixed = max(1, used // 4)
        shifted = fixed + (places - fixed + rotation * (used - fixed)) % max(1, number_of - fixed)
        return jnp.zeros((number_of,), jnp.int32).at[sequence[jnp.where(places < fixed, places, shifted)]].set(jnp.asarray(sizes, jnp.int32))

    sizes = jnp.where(number % 4 == 0, named(packed, number // 4), named(usual, number - number // 4 - 1))
    mixed = jax.random.permutation(jax.random.fold_in(own, 3), number_of)
    donor, sink = mixed[0:number_of // 2 * 2:2], mixed[1:number_of // 2 * 2:2]
    slack = jnp.minimum(sizes[donor] - 1, reach - sizes[sink]) // 2
    slack = jnp.where((donor == sequence[0]) | (sink == sequence[0]) | (sizes[sink] == 0), 0, jnp.maximum(slack, 0))
    shifted = jax.random.randint(jax.random.fold_in(own, 4), (number_of // 2,), 0, 1 << 20) % (slack + 1)
    sizes = sizes.at[donor].add(-shifted).at[sink].add(shifted)
    items = jnp.searchsorted(jnp.cumsum(sizes), jnp.arange(rows * top), side="right").astype(jnp.int32)
    grid = items.reshape(top, rows).T
    grid = grid[jax.random.permutation(jax.random.fold_in(own, 1), rows)]
    rotation = jax.random.randint(jax.random.fold_in(own, 2), (rows, 1), 0, top)
    return jnp.take_along_axis(grid, (jnp.arange(top)[None, :] + rotation) % top, axis=1)


def load_shares(count, total, limit, lean, full):
    loads = [(1 << 20) // math.isqrt(grade ** lean) + 1 for grade in range(1, count + 1)]
    largest = limit if full else min(limit, max(-(-total // count), total * loads[0] // sum(loads)))
    least = 1 if total - largest >= count - 1 else 0
    counts, spare = [largest] + [least] * (count - 1), total - largest - least * (count - 1)
    while spare > 0:
        candidates = [i for i in range(1, count) if counts[i] < largest] or [i for i in range(1, count) if counts[i] < limit]
        pool, left = sum([loads[i] for i in candidates]), spare
        for i in candidates:
            more = min(limit - counts[i], max(1, left * loads[i] // pool), spare)
            counts[i] = counts[i] + more
            spare = spare - more
    return np.array(counts)


def gaussian(key, extent, deviation, most, pieces=(), kind=jnp.bfloat16):
    entries = deviation * jax.random.normal(key, extent, jnp.float32)
    if pieces:
        entries = entries * shard_levels(key, extent, pieces, -0.22, 0.18)
    return jnp.clip(entries, -most, most).astype(kind)


def setup_inputs(seed: int = 0) -> dict:
    arg_keys = jax.random.split(jax.random.key(seed), 18)
    attn_in = gaussian(arg_keys[0], (TOKENS, D), 1.0, 6.0, ((0, 32),))
    mix_gain = jnp.clip(1.0 + 0.18 * jax.random.normal(arg_keys[1], (D,), jnp.float32), 0.1, 1.9)
    query_weight = gaussian(arg_keys[2], (D, HEADS * HD), D ** -0.5, 0.125, ((1, 16),))
    key_weight = gaussian(arg_keys[3], (D, HEADS * HD), D ** -0.5, 0.125, ((1, 16),))
    value_weight = gaussian(arg_keys[4], (D, HEADS * HD), D ** -0.5, 0.125, ((1, 16),))
    query_gain = draw_query_gain(jax.random.fold_in(arg_keys[17], 71), 0)
    key_gain = draw_key_gain(jax.random.fold_in(arg_keys[17], 71), 0)
    log_cache = draw_log_cache(jax.random.fold_in(arg_keys[17], 71), 0)
    head_gain = jnp.clip(1.0 + 0.18 * jax.random.normal(arg_keys[8], (HEADS * HD,), jnp.float32), 0.1, 1.9)
    out_weight = gaussian(arg_keys[9], (HEADS * HD, D), (HEADS * HD) ** -0.5, 0.1875, ((1, 16),))
    moe_in = gaussian(arg_keys[10], (TOKENS2, D), 1.0, 6.0, ((0, 32),))
    moe_gain = jnp.clip(1.0 + 0.18 * jax.random.normal(arg_keys[11], (D,), jnp.float32), 0.1, 1.9)
    routes_keys = jax.random.split(jax.random.fold_in(arg_keys[12], 1), TOKENS2 // TOK_MOE)
    routes_turns = jax.random.permutation(jax.random.fold_in(arg_keys[12], 3), TOKENS2 // TOK_MOE)
    routes = jax.vmap(lambda own, number: assign_block(jax.random.fold_in(arg_keys[12], 2), own, number, TOK_MOE, EXPERTS, TOPK, CAP, 1))(routes_keys, routes_turns).reshape((TOKENS2, TOPK))
    route_weight = jnp.clip(jnp.exp(math.log(1.0) - 1.3862944 * jax.random.uniform(arg_keys[13], (TOKENS2, TOPK), jnp.float32) ** shard_levels(arg_keys[13], (TOKENS2, TOPK), ((0, 32),), -0.2, 0.2)), 0.25, 1.0)
    expert_gate = gaussian(arg_keys[14], (EXPERTS, D, FFE), D ** -0.5, 0.125, ((0, 32), (2, 16)))
    expert_up = gaussian(arg_keys[15], (EXPERTS, D, FFE), D ** -0.5, 0.125, ((0, 32), (2, 16)))
    expert_down = gaussian(arg_keys[16], (EXPERTS, FFE, D), FFE ** -0.5, 0.1875, ((0, 32), (1, 16)))
    return {"attn_in": attn_in, "mix_gain": mix_gain, "query_weight": query_weight, "key_weight": key_weight, "value_weight": value_weight, "query_gain": query_gain, "key_gain": key_gain, "log_cache": log_cache, "head_gain": head_gain, "out_weight": out_weight, "moe_in": moe_in, "moe_gain": moe_gain, "routes": routes, "route_weight": route_weight, "expert_gate": expert_gate, "expert_up": expert_up, "expert_down": expert_down}


epsilon = 1e-06

def row_norm(inputs, gain_vec):
    floats = inputs.astype(jnp.float32)
    scaled = floats * lax.rsqrt(lax.optimization_barrier(jnp.mean(floats * floats, axis=-1, keepdims=True)) + epsilon)
    return scaled * gain_vec.astype(jnp.float32)

def reference(attn_in, mix_gain, query_weight, key_weight, value_weight, query_gain, key_gain, log_cache, head_gain, out_weight, moe_in, moe_gain, routes, route_weight, expert_gate, expert_up, expert_down):
    seq_len = attn_in.shape[0]
    normed = row_norm(attn_in, mix_gain).astype(jnp.bfloat16)

    def project(weight):
        return jnp.dot(normed, weight, preferred_element_type=jnp.float32).reshape(seq_len, HEADS, HD)
    queries = row_norm(project(query_weight), query_gain).astype(jnp.bfloat16)
    key_rows = row_norm(project(key_weight), key_gain).astype(jnp.bfloat16)
    value_rows = project(value_weight).astype(jnp.bfloat16)
    block_len = math.gcd(seq_len, 512)
    block_count = seq_len // block_len
    positions = jnp.arange(seq_len, dtype=jnp.int32)
    score_scale = HD ** (-0.5)

    def one_block(flat_index):
        head_index = flat_index // block_count
        block_begin = flat_index % block_count * block_len
        head_queries = lax.dynamic_index_in_dim(queries, head_index, 1, False)
        query_block = lax.dynamic_slice_in_dim(head_queries, block_begin, block_len, 0)
        head_keys = lax.dynamic_index_in_dim(key_rows, head_index, 1, False)
        head_values = lax.dynamic_index_in_dim(value_rows, head_index, 1, False)
        head_gates = lax.dynamic_index_in_dim(log_cache, head_index, 1, False)
        query_gates = lax.dynamic_slice_in_dim(head_gates, block_begin, block_len, 0)
        scores = jnp.dot(query_block, head_keys.T, preferred_element_type=jnp.float32) * score_scale
        scores = scores + query_gates[:, None] - head_gates[None, :]
        query_pos = block_begin + jnp.arange(block_len, dtype=jnp.int32)
        causal = positions[None, :] <= query_pos[:, None]
        scores = jnp.where(causal, scores, -jnp.inf)
        row_max = lax.optimization_barrier(jnp.max(scores, axis=1, keepdims=True))
        expo_scores = jnp.exp(scores - row_max)
        denominator = lax.optimization_barrier(jnp.sum(expo_scores, axis=1, keepdims=True))
        mixed_rows = jnp.dot(expo_scores.astype(jnp.bfloat16), head_values, preferred_element_type=jnp.float32)
        return mixed_rows / denominator
    blocks = lax.map(one_block, jnp.arange(HEADS * block_count, dtype=jnp.int32))
    attended = jnp.transpose(blocks.reshape(HEADS, seq_len, HD), (1, 0, 2))
    head_out = row_norm(attended, head_gain.reshape(HEADS, HD)).astype(jnp.bfloat16).reshape(seq_len, HEADS * HD)
    mixer_out = jnp.dot(head_out, out_weight, preferred_element_type=jnp.float32).astype(jnp.bfloat16)
    moe_normed = row_norm(moe_in, moe_gain).astype(jnp.bfloat16)
    flat_routes = routes.reshape(-1)
    slot_total = N_EP * CAP

    def one_expert(expert):
        chosen = flat_routes == expert
        picked = jnp.nonzero(chosen, size=slot_total, fill_value=0)[0].astype(jnp.int32)
        alive_mask = (jnp.arange(slot_total, dtype=jnp.int32) < jnp.sum(chosen.astype(jnp.int32))).astype(jnp.float32)
        token_rows = moe_normed[picked // TOPK]
        gate_w = lax.dynamic_index_in_dim(expert_gate, expert, 0, False)
        up_w = lax.dynamic_index_in_dim(expert_up, expert, 0, False)
        down_w = lax.dynamic_index_in_dim(expert_down, expert, 0, False)
        gate_sum = jnp.dot(token_rows, gate_w, preferred_element_type=jnp.float32)
        up_sum = jnp.dot(token_rows, up_w, preferred_element_type=jnp.float32)
        hidden = (jax.nn.silu(gate_sum) * up_sum).astype(jnp.bfloat16)
        expert_rows = jnp.dot(hidden, down_w, preferred_element_type=jnp.float32).astype(jnp.bfloat16)
        return (picked, alive_mask, expert_rows)
    picked, alive_mask, expert_rows = lax.map(one_expert, jnp.arange(EXPERTS, dtype=jnp.int32))
    flat_weight = route_weight.reshape(-1)
    scaled_rows = expert_rows.astype(jnp.float32) * (flat_weight[picked] * alive_mask)[:, :, None]
    token_index = (picked // TOPK).reshape(-1)
    moe_sum = jnp.zeros((flat_routes.shape[0] // TOPK, D), jnp.float32).at[token_index].add(scaled_rows.reshape(-1, D))
    moe_out = moe_sum.astype(jnp.bfloat16)
    return (mixer_out, moe_out)
```

```python
import functools

import jax
import jax.numpy as jnp
from jax import lax
from jax.experimental import pallas as pl
from jax.experimental.pallas import tpu as pltpu
from jax.sharding import PartitionSpec as P

HD = 64
EPS = 1e-06
GR = 16
KR = HD + GR
BR = KR + HD
SIDE = 4
SLOT = 16
MESH = pl.DeviceIdType.MESH
F32 = jnp.float32
BF16 = jnp.bfloat16


def dot(a, b, dims=((1,), (0,))):
    return lax.dot_general(a, b, (dims, ((), ())), preferred_element_type=F32)


def iota(shape, dim):
    return lax.broadcasted_iota(jnp.int32, shape, dim)


def norm_rows(x, gain):
    return x * lax.rsqrt(jnp.mean(x * x, axis=-1, keepdims=True) + EPS) * gain


def to_row(col):
    n = col.shape[0]
    eye = iota((n, n), 0) == iota((n, n), 1)
    return jnp.sum(jnp.where(eye, col, 0.0), axis=0, keepdims=True)


def to_col(row):
    n = row.shape[1]
    eye = iota((n, n), 0) == iota((n, n), 1)
    return jnp.sum(jnp.where(eye, row, 0.0), axis=1, keepdims=True)


def local(src, dst, sem):
    return pltpu.make_async_copy(src, dst, sem)


def send(src, dst, ssem, rsem, ep, tp):
    return pltpu.make_async_remote_copy(
        src_ref=src,
        dst_ref=dst,
        send_sem=ssem,
        recv_sem=rsem,
        device_id=(ep, tp),
        device_id_type=MESH,
    )


class Torus:
    def __init__(self, colour, ep, tp):
        y, x = lax.div(tp, SIDE), lax.rem(tp, SIDE)
        self.ep, self.tp, self.colour = ep, tp, colour
        self.a, self.b = (y, x) if colour == 0 else (x, y)

    def at(self, a, b):
        a, b = lax.rem(a + SIDE, SIDE), lax.rem(b + SIDE, SIDE)
        return a * SIDE + b if self.colour == 0 else b * SIDE + a


class Gather:
    def __init__(self, torus, buf, half, ssem, rsem):
        self.t, self.buf, self.half, self.ss, self.rs = torus, buf, half, ssem, rsem
        a, b = torus.a, torus.b
        self.am, self.ap, self.ao = (lax.rem(a + k, SIDE) for k in (3, 1, 2))
        self.bm, self.bp, self.bo = (lax.rem(b + k, SIDE) for k in (3, 1, 2))
        t, h = torus, half
        buf = self.buf
        lo, hi = pl.ds(0, h), pl.ds(h, h)
        lo2, hi2 = pl.ds(0, SIDE // 2), pl.ds(SIDE // 2, SIDE // 2)
        right_b, left_b = t.at(a, b + 1), t.at(a, b - 1)
        right_a, left_a = t.at(a + 1, b), t.at(a - 1, b)
        self.out = [
            (buf.at[a, b], right_b),
            (buf.at[a, b], left_b),
            (buf.at[a, self.bm, lo], right_b),
            (buf.at[a, self.bp, hi], left_b),
            (buf.at[a], right_a),
            (buf.at[a], left_a),
            (buf.at[self.am, lo2], right_a),
            (buf.at[self.ap, hi2], left_a),
        ]
        self.inn = [
            buf.at[a, self.bm],
            buf.at[a, self.bp],
            buf.at[a, self.bo, lo],
            buf.at[a, self.bo, hi],
            buf.at[self.am],
            buf.at[self.ap],
            buf.at[self.ao, lo2],
            buf.at[self.ao, hi2],
        ]

    def start(self, k):
        src, to = self.out[k]
        send(src, src, self.ss.at[k], self.rs.at[k], self.t.ep, to).start()

    def arrive(self, k):
        dst = self.inn[k]
        send(dst, dst, self.ss.at[k], self.rs.at[k], self.t.ep, self.t.tp).wait_recv()

    def sent(self):
        for k in range(8):
            src, to = self.out[k]
            send(src, src, self.ss.at[k], self.rs.at[k], self.t.ep, to).wait_send()

    def stages(self):
        return [
            lambda: [self.start(0), self.start(1)],
            lambda: [self.arrive(0), self.start(2), self.arrive(1), self.start(3)],
            lambda: [self.arrive(2), self.arrive(3), self.start(4), self.start(5)],
            lambda: [self.arrive(4), self.start(6), self.arrive(5), self.start(7)],
            lambda: [self.arrive(6), self.arrive(7), self.sent()],
        ]


class Reduce:
    def __init__(self, torus, part, ra, rb, sa, sb, own, ssem, rsem):
        self.t, self.part, self.ra, self.rb, self.sa, self.sb, self.own = (
            torus,
            part,
            ra,
            rb,
            sa,
            sb,
            own,
        )
        self.ss, self.rs = ssem, rsem
        a, b = torus.a, torus.b
        self.am, self.ap, self.ao = (lax.rem(a + k, SIDE) for k in (3, 1, 2))
        self.bm, self.bp, self.bo = (lax.rem(b + k, SIDE) for k in (3, 1, 2))
        t = torus
        h = own.shape[1] // 2
        self.h = h
        lo2, hi2 = pl.ds(0, SIDE // 2), pl.ds(SIDE // 2, SIDE // 2)
        lo, hi = pl.ds(0, h), pl.ds(h, h)
        right_b, left_b = t.at(a, b + 1), t.at(a, b - 1)
        right_a, left_a = t.at(a + 1, b), t.at(a - 1, b)
        self.out = [
            (part.at[self.ao, lo2], ra.at[2, lo2], right_a),
            (part.at[self.ao, hi2], ra.at[2, hi2], left_a),
            (sa.at[0], ra.at[0], right_a),
            (sa.at[1], ra.at[1], left_a),
            (own.at[self.bo, lo], rb.at[2, lo], right_b),
            (own.at[self.bo, hi], rb.at[2, hi], left_b),
            (sb.at[0], rb.at[0], right_b),
            (sb.at[1], rb.at[1], left_b),
        ]

    def start(self, k):
        src, dst, to = self.out[k]
        send(src, dst, self.ss.at[k], self.rs.at[k], self.t.ep, to).start()

    def arrive(self, k):
        _, dst, to = self.out[k]
        send(dst, dst, self.ss.at[k], self.rs.at[k], self.t.ep, to).wait_recv()

    def sent(self):
        for k in range(8):
            src, dst, to = self.out[k]
            send(src, dst, self.ss.at[k], self.rs.at[k], self.t.ep, to).wait_send()

    def first(self):
        self.start(0)
        self.start(1)

    def second(self):
        p, ra, sa = self.part, self.ra, self.sa
        half = SIDE // 2
        sa[0, half:] = p[self.ap, half:]
        sa[1, :half] = p[self.am, :half]
        self.arrive(0)
        sa[0, :half] = (p[self.ap, :half].astype(F32) + ra[2, :half].astype(F32)).astype(BF16)
        self.start(2)
        self.arrive(1)
        sa[1, half:] = (p[self.am, half:].astype(F32) + ra[2, half:].astype(F32)).astype(BF16)
        self.start(3)

    def third(self):
        p, ra = self.part, self.ra
        self.arrive(2)
        self.arrive(3)

        def one(j, _):
            self.own[j] = (
                p[self.t.a, j].astype(F32) + ra[0, j].astype(F32) + ra[1, j].astype(F32)
            ).astype(BF16)
            return 0

        lax.fori_loop(0, SIDE, one, 0)
        self.start(4)
        self.start(5)

    def fourth(self):
        o, rb, sb, h = self.own, self.rb, self.sb, self.h
        sb[0, h:] = o[self.bp, h:]
        sb[1, :h] = o[self.bm, :h]
        self.arrive(4)
        sb[0, :h] = (o[self.bp, :h].astype(F32) + rb[2, :h].astype(F32)).astype(BF16)
        self.start(6)
        self.arrive(5)
        sb[1, h:] = (o[self.bm, h:].astype(F32) + rb[2, h:].astype(F32)).astype(BF16)
        self.start(7)

    def result(self):
        self.arrive(6)
        self.arrive(7)
        r = (
            self.own[self.t.b].astype(F32) + self.rb[0].astype(F32) + self.rb[1].astype(F32)
        ).astype(BF16)
        self.sent()
        return r


class Exchange:
    def __init__(self, ep, tp, n, src, dst, ssem, rsem):
        self.ep, self.tp, self.n = ep, tp, n
        self.src, self.dst, self.ss, self.rs = src, dst, ssem, rsem

    def start(self):
        self.dst[self.ep] = self.src[self.ep]

        def one(i, _):
            step = lax.select(lax.rem(i, 2) == 1, lax.div(i + 1, 2), self.n - lax.div(i, 2))
            peer = lax.rem(self.ep + step, self.n)
            send(
                self.src.at[peer],
                self.dst.at[self.ep],
                self.ss.at[peer],
                self.rs.at[self.ep],
                peer,
                self.tp,
            ).start()
            return 0

        lax.fori_loop(1, self.n, one, 0)

    def arrive(self):
        def one(i, _):
            peer = lax.rem(self.ep + i, self.n)
            d = send(
                self.src.at[peer],
                self.dst.at[peer],
                self.ss.at[peer],
                self.rs.at[peer],
                peer,
                self.tp,
            )
            d.wait_recv()
            d.wait_send()
            return 0

        lax.fori_loop(1, self.n, one, 0)


def kernel(
    n_ep,
    n_tp,
    x_h,
    mix_gain,
    wq_h,
    wk_h,
    wv_h,
    q_gain,
    k_gain,
    gates,
    h_gain,
    wo_h,
    mx_h,
    moe_gain,
    routes,
    rweight,
    wg_h,
    wu_h,
    wd_h,
    mixer_out,
    moe_out,
    x,
    nx,
    wq,
    wk,
    wv,
    wo,
    mx,
    wg,
    wu,
    wd,
    kv,
    qa,
    acc,
    mx_run,
    hg0,
    hg1,
    sendb,
    recvb,
    retb,
    backb,
    onehot,
    g0,
    g1,
    part0,
    part1,
    ra0,
    ra1,
    rb0,
    rb1,
    sa0,
    sa1,
    sb0,
    sb1,
    own0,
    own1,
    load_sem,
    kv_recv,
    up_send,
    dn_send,
    sib_send,
    hg_s,
    hg_r,
    mg_s,
    mg_r,
    rd_s,
    rd_r,
    d_s,
    d_r,
    b_s,
    b_r,
):
    ep, tp = lax.axis_index("ep"), lax.axis_index("tp")
    z, core = lax.div(ep, 2), lax.rem(ep, 2)
    nz = n_ep // 2
    ups, dns = nz // 2, nz - 1 - nz // 2
    tq = x.shape[0]
    half_t = tq // 2

    loads = [
        local(s, d, load_sem.at[i])
        for i, (s, d) in enumerate(
            [
                (mx_h, mx),
                (x_h, x),
                (wq_h, wq),
                (wk_h, wk),
                (wv_h, wv),
                (wg_h.at[0], wg),
                (wu_h.at[0], wu),
                (wd_h.at[0], wd),
                (wo_h, wo),
            ]
        )
    ]
    for d in loads:
        d.start()

    barrier = pltpu.get_barrier_semaphore()

    def greet_ep(i, _):
        pl.semaphore_signal(
            barrier, inc=1, device_id=(lax.rem(ep + i, n_ep), tp), device_id_type=MESH
        )
        return 0

    def greet_tp(i, _):
        pl.semaphore_signal(
            barrier, inc=1, device_id=(ep, lax.rem(tp + i, n_tp)), device_id_type=MESH
        )
        return 0

    lax.fori_loop(1, n_ep, greet_ep, 0)
    lax.fori_loop(1, n_tp, greet_tp, 0)

    toks = mx.shape[0]
    slots = n_ep * SLOT
    loads[0].wait()
    r_col = routes[...].astype(F32)
    r_rows = [to_row(r_col[:, k : k + 1]) for k in range(2)]
    experts = iota((n_ep, toks), 0).astype(F32)
    hot = [(experts == r).astype(F32) for r in r_rows]
    before = (iota((toks, toks), 0) < iota((toks, toks), 1)).astype(BF16)
    counts = dot((hot[0] + hot[1]).astype(BF16), before)
    for k in range(2):
        order = jnp.sum(hot[k] * counts, axis=0, keepdims=True)
        slot = (r_rows[k] * SLOT + order).astype(jnp.int32)
        onehot[k] = (iota((slots, toks), 0) == slot).astype(F32).astype(BF16)
    mxf = mx[...].astype(F32)
    mscale = lax.rsqrt(jnp.mean(mxf * mxf, axis=-1, keepdims=True) + EPS)
    cols = pl.ds(pl.multiple_of(tp * 128, 128), 128)
    mslice = (mx[:, cols].astype(F32) * mscale * moe_gain[:, cols]).astype(BF16)
    both = (onehot[0].astype(F32) + onehot[1].astype(F32)).astype(BF16)
    sendb[...] = dot(both, mslice).astype(BF16).reshape(n_ep, SLOT, 128)

    loads[1].wait()

    def norm_some(i, _):
        rows = pl.ds(pl.multiple_of(i * 64, 64), 64)
        nx[rows, :] = norm_rows(x[rows, :].astype(F32), mix_gain[...]).astype(BF16)
        return 0

    lax.fori_loop(0, tq // 64, norm_some, 0)
    for d in loads[2:5]:
        d.wait()
    n_all = nx[...]
    q = norm_rows(dot(n_all, wq[...]), q_gain[...]) * (HD**-0.5)
    k = norm_rows(dot(n_all, wk[...]), k_gain[...])
    v = dot(n_all, wv[...])
    qa[0:HD, :] = q.T.astype(BF16)
    ridx = iota((GR, tq), 0)
    qa[HD:KR, :] = jnp.where(ridx < 3, -1.0, 0.0).astype(BF16)
    g = gates[...]
    ghi = g.astype(BF16).astype(F32)
    gmid = (g - ghi).astype(BF16).astype(F32)
    glo = g - ghi - gmid
    grow = jnp.where(
        ridx == 0,
        ghi,
        jnp.where(ridx == 1, gmid, jnp.where(ridx == 2, glo, jnp.where(ridx == 3, 1.0, 0.0))),
    ).astype(BF16)
    kt, vt = k.T.astype(BF16), v.T.astype(BF16)
    for c in range(2):
        cc = slice(c * half_t, (c + 1) * half_t)
        kv[ep, c, 0:HD, :] = kt[:, cc]
        kv[ep, c, HD:KR, :] = grow[:, cc]
        kv[ep, c, KR:BR, :] = vt[:, cc]

    pl.semaphore_wait(barrier, n_ep - 1 + n_tp - 1)

    dispatch = Exchange(ep, tp, n_ep, sendb, recvb, d_s, d_r)
    dispatch.start()

    def hop(slot, c, to_ep, ssem):
        return send(kv.at[slot, c], kv.at[slot, c], ssem, kv_recv.at[slot, c], to_ep, tp)

    up_ep = lax.rem(z + 1, nz) * 2 + core
    dn_ep = lax.rem(z + nz - 1, nz) * 2 + core
    sib_ep = z * 2 + 1 - core

    def slot_of(step, whose):
        return lax.rem(z + step + nz, nz) * 2 + whose

    for c in range(2):
        hop(ep, c, up_ep, up_send.at[0, c]).start()
        hop(ep, c, dn_ep, dn_send.at[0, c]).start()
        hop(ep, c, sib_ep, sib_send.at[ep, c]).start()

    def flash(slot, diagonal=False):
        s = [dot(kv[slot, c, 0:KR, :], qa[...], ((0,), (0,))) for c in range(2)]
        if diagonal:
            s = [
                jnp.where(
                    iota((half_t, tq), 0) + c * half_t <= iota((half_t, tq), 1), s[c], -1e30
                )
                for c in range(2)
            ]
        top = jnp.maximum(
            jnp.max(s[0], axis=0, keepdims=True), jnp.max(s[1], axis=0, keepdims=True)
        )
        if diagonal:
            new = top
        else:
            old = mx_run[...]
            new = jnp.maximum(old, top)
        got = None
        for c in range(2):
            w = jnp.exp(s[c] - new).astype(BF16)
            o = dot(kv[slot, c, HD:BR, :], w)
            got = o if got is None else got + o
        if diagonal:
            acc[...] = got
        else:
            acc[...] = acc[...] * jnp.exp(old - new) + got
        mx_run[...] = new

    flash(ep, diagonal=True)

    def take(slot):
        @pl.when(slot < ep)
        def _():
            flash(slot)

    def wait_block(slot, c):
        hop(slot, c, sib_ep, sib_send.at[slot, c]).wait_recv()

    t0, t1 = Torus(0, ep, tp), Torus(1, ep, tp)
    rows = g0.shape[2]
    mg = [
        Gather(t0, g0, rows // 2, mg_s.at[0], mg_r.at[0]),
        Gather(t1, g1, rows // 2, mg_s.at[1], mg_r.at[1]),
    ]
    rd = [
        Reduce(t0, part0, ra0, rb0, sa0, sb0, own0, rd_s.at[0], rd_r.at[0]),
        Reduce(t1, part1, ra1, rb1, sa1, sb1, own1, rd_s.at[1], rd_r.at[1]),
    ]
    cap = 2 * rows // n_ep
    returns = Exchange(ep, tp, n_ep, retb, backb, b_s, b_r)

    def pick(rows_out, rows_in, wide_first):
        wide, dense = (0, 1) if wide_first else (1, 0)
        w, d = iota((rows_out, rows_in), wide), iota((rows_out, rows_in), dense)
        i = lax.rem(w, SLOT)
        hit = jnp.logical_and(lax.div(w, SLOT) * cap + i == d, i < cap)
        return hit.astype(F32).astype(BF16)

    def pack_rows():
        dispatch.arrive()
        packed = dot(
            pick(2 * rows, slots, False), recvb[...].reshape(slots, 128)
        ).astype(BF16)
        g0[t0.a, t0.b] = packed[:rows]
        g1[t1.a, t1.b] = packed[rows:]
        for m in mg:
            m.stages()[0]()

    def experts_now():
        for d in loads[5:8]:
            d.wait()
        for m, buf, part in ((mg[0], g0, part0), (mg[1], g1, part1)):
            m.stages()[4]()
            gs = us = None
            for a in range(SIDE):
                for b in range(SIDE):
                    t = a * SIDE + b if m.t.colour == 0 else b * SIDE + a
                    blk = buf[a, b]
                    p = dot(blk, wg[t * 128 : (t + 1) * 128, :])
                    r = dot(blk, wu[t * 128 : (t + 1) * 128, :])
                    gs = p if gs is None else gs + p
                    us = r if us is None else us + r
            hidden = (gs / (1.0 + jnp.exp(-gs)) * us).astype(BF16)
            for a in range(SIDE):
                for b in range(SIDE):
                    t = a * SIDE + b if m.t.colour == 0 else b * SIDE + a
                    part[a, b] = dot(hidden, wd[:, t * 128 : (t + 1) * 128]).astype(BF16)
        for r in rd:
            r.first()

    def give_back():
        summed = jnp.concatenate([rd[0].result(), rd[1].result()], axis=0)
        retb[...] = (
            dot(pick(slots, 2 * rows, True), summed).astype(BF16).reshape(n_ep, SLOT, 128)
        )
        returns.start()

    hooks = {
        3: pack_rows,
        4: lambda: [m.stages()[1]() for m in mg],
        5: lambda: [m.stages()[2]() for m in mg],
        6: lambda: [m.stages()[3]() for m in mg],
        8: experts_now,
    }

    def ring(s, _):
        up, dn = slot_of(-s, core), slot_of(s, core)
        for c in range(2):
            wait_block(up, c)

            @pl.when(s < ups)
            def _():
                hop(up, c, up_ep, up_send.at[s, c]).start()

            hop(up, c, sib_ep, sib_send.at[up, c]).start()

            @pl.when(s <= dns)
            def _():
                wait_block(dn, c)

                @pl.when(s < dns)
                def _():
                    hop(dn, c, dn_ep, dn_send.at[s, c]).start()

                hop(dn, c, sib_ep, sib_send.at[dn, c]).start()

            if c == 0:
                def handed(i, _):
                    far = slot_of(lax.select(i == 0, 1 - s, s - 1), 1 - core)

                    @pl.when(jnp.logical_or(i == 0, s >= 2))
                    def _():
                        wait_block(far, 0)
                        wait_block(far, 1)
                        take(far)

                    return 0

                lax.fori_loop(0, 2, handed, 0)

        def came(i, _):
            near = slot_of(lax.select(i == 0, -s, s), core)

            @pl.when(jnp.logical_or(i == 0, s <= dns))
            def _():
                take(near)

            return 0

        lax.fori_loop(0, 2, came, 0)
        for at, hook in hooks.items():

            @pl.when(s == at)
            def _():
                hook()

        return 0

    lax.fori_loop(1, ups + 1, ring, 0)
    last = slot_of(-ups, 1 - core)
    wait_block(last, 0)
    wait_block(last, 1)
    take(last)

    for r in rd:
        r.second()
    att = acc[GR:, :] / acc[3:4, :]
    att = att * lax.rsqrt(jnp.mean(att * att, axis=0, keepdims=True) + EPS)
    head = (att * to_col(h_gain[...])).astype(BF16)
    hg0[t0.a, t0.b] = head[:, :half_t]
    hg1[t1.a, t1.b] = head[:, half_t:]
    hg = [
        Gather(t0, hg0, HD // 2, hg_s.at[0], hg_r.at[0]),
        Gather(t1, hg1, HD // 2, hg_s.at[1], hg_r.at[1]),
    ]
    for m in hg:
        m.stages()[0]()
    for r in rd:
        r.third()
    for m in hg:
        m.stages()[1]()
    for r in rd:
        r.fourth()
    for m in hg:
        m.stages()[2]()
    give_back()
    for m in hg:
        m.stages()[3]()
    loads[8].wait()
    for i, (m, buf) in enumerate(((hg[0], hg0), (hg[1], hg1))):
        m.stages()[4]()
        o = None
        for a in range(SIDE):
            for b in range(SIDE):
                t = a * SIDE + b if i == 0 else b * SIDE + a
                p = dot(buf[a, b], wo[t * HD : (t + 1) * HD, :], ((0,), (0,)))
                o = p if o is None else o + p
        mixer_out[i * half_t : (i + 1) * half_t, :] = o.astype(BF16)

    returns.arrive()
    back = backb[...].reshape(slots, 128)
    total = None
    for k in range(2):
        got = dot(onehot[k], back, ((0,), (0,))) * rweight[:, k : k + 1]
        total = got if total is None else total + got
    moe_out[...] = total.astype(BF16)

    def up_done(s, _):
        for c in range(2):
            hop(slot_of(-s, core), c, up_ep, up_send.at[s, c]).wait_send()
        return 0

    def dn_done(s, _):
        for c in range(2):
            hop(slot_of(s, core), c, dn_ep, dn_send.at[s, c]).wait_send()
        return 0

    def sib_done(i, _):
        for c in range(2):
            slot = i * 2 + core
            hop(slot, c, sib_ep, sib_send.at[slot, c]).wait_send()
        return 0

    lax.fori_loop(0, ups, up_done, 0)
    lax.fori_loop(0, dns, dn_done, 0)
    lax.fori_loop(0, nz, sib_done, 0)


def body(
    n_ep,
    n_tp,
    attn_in,
    mix_gain,
    query_weight,
    key_weight,
    value_weight,
    query_gain,
    key_gain,
    log_cache,
    head_gain,
    out_weight,
    moe_in,
    moe_gain,
    routes,
    route_weight,
    expert_gate,
    expert_up,
    expert_down,
):
    tq, d = attn_in.shape
    toks = moe_in.shape[0]
    cap = 3 * toks * routes.shape[1] // (2 * n_ep)
    rows = n_ep * cap // 2
    vm = pl.BlockSpec(memory_space=pltpu.VMEM)
    hbm = pl.BlockSpec(memory_space=pl.ANY)
    dma = pltpu.SemaphoreType.DMA

    def v(*shape, dtype=BF16):
        return pltpu.VMEM(shape, dtype)

    nz = n_ep // 2
    scratch = [
        v(tq, d),
        v(tq, d),
        v(d, HD),
        v(d, HD),
        v(d, HD),
        v(n_tp * HD, 128),
        v(toks, d),
        v(d, 64),
        v(d, 64),
        v(64, d),
        v(n_ep, 2, BR, tq // 2),
        v(KR, tq),
        v(GR + HD, tq, dtype=F32),
        v(1, tq, dtype=F32),
        v(SIDE, SIDE, HD, tq // 2),
        v(SIDE, SIDE, HD, tq // 2),
        v(n_ep, SLOT, 128),
        v(n_ep, SLOT, 128),
        v(n_ep, SLOT, 128),
        v(n_ep, SLOT, 128),
        v(2, n_ep * SLOT, toks),
        v(SIDE, SIDE, rows, 128),
        v(SIDE, SIDE, rows, 128),
        v(SIDE, SIDE, rows, 128),
        v(SIDE, SIDE, rows, 128),
        v(3, SIDE, rows, 128),
        v(3, SIDE, rows, 128),
        v(3, rows, 128),
        v(3, rows, 128),
        v(2, SIDE, rows, 128),
        v(2, SIDE, rows, 128),
        v(2, rows, 128),
        v(2, rows, 128),
        v(SIDE, rows, 128),
        v(SIDE, rows, 128),
        dma((9,)),
        dma((n_ep, 2)),
        dma((nz, 2)),
        dma((nz, 2)),
        dma((n_ep, 2)),
        dma((2, 8)),
        dma((2, 8)),
        dma((2, 8)),
        dma((2, 8)),
        dma((2, 8)),
        dma((2, 8)),
        dma((n_ep,)),
        dma((n_ep,)),
        dma((n_ep,)),
        dma((n_ep,)),
    ]
    return pl.pallas_call(
        functools.partial(kernel, n_ep, n_tp),
        out_shape=(
            jax.ShapeDtypeStruct((tq, 128), BF16),
            jax.ShapeDtypeStruct((toks, 128), BF16),
        ),
        in_specs=[hbm, vm, hbm, hbm, hbm, vm, vm, vm, vm, hbm, hbm, vm, vm, vm, hbm, hbm, hbm],
        out_specs=(vm, vm),
        scratch_shapes=scratch,
        compiler_params=pltpu.CompilerParams(
            collective_id=0, has_side_effects=True, vmem_limit_bytes=60 * 1024 * 1024
        ),
    )(
        attn_in,
        mix_gain.reshape(1, -1),
        query_weight,
        key_weight,
        value_weight,
        query_gain.reshape(1, -1),
        key_gain.reshape(1, -1),
        log_cache.reshape(1, -1),
        head_gain.reshape(1, -1),
        out_weight,
        moe_in,
        moe_gain.reshape(1, -1),
        routes,
        route_weight,
        expert_gate,
        expert_up,
        expert_down,
    )


def solution(mesh):
    n_ep, n_tp = mesh.shape["ep"], mesh.shape["tp"]
    in_specs = (
        P("ep", None),
        P(),
        P(None, "tp"),
        P(None, "tp"),
        P(None, "tp"),
        P(),
        P(),
        P("ep", "tp"),
        P("tp"),
        P(None, "tp"),
        P("ep", None),
        P(),
        P("ep", None),
        P("ep", None),
        P("ep", None, "tp"),
        P("ep", None, "tp"),
        P("ep", "tp", None),
    )
    out_specs = (P("ep", "tp"), P("ep", "tp"))
    return jax.shard_map(
        functools.partial(body, n_ep, n_tp),
        mesh=mesh,
        in_specs=in_specs,
        out_specs=out_specs,
        check_vma=False,
    )
```

```python
import functools

import jax
import jax.numpy as jnp
from jax import lax
from jax.experimental import pallas as pl
from jax.experimental.pallas import tpu as pltpu
from jax.sharding import PartitionSpec as P

HD = 64
EPS = 1e-06
GR = 8
KR = HD + GR
BR = KR + HD
SIDE = 4
SLOT = 16
NCH = 4
NH = NCH // 2
MESH = pl.DeviceIdType.MESH
F32 = jnp.float32
BF16 = jnp.bfloat16


def dot(a, b, dims=((1,), (0,))):
    return lax.dot_general(a, b, (dims, ((), ())), preferred_element_type=F32)


def iota(shape, dim):
    return lax.broadcasted_iota(jnp.int32, shape, dim)


def norm_rows(x, gain):
    return x * lax.rsqrt(jnp.mean(x * x, axis=-1, keepdims=True) + EPS) * gain


def norm_cols(x, gain):
    return x * lax.rsqrt(jnp.mean(x * x, axis=0, keepdims=True) + EPS) * gain


def to_col(row):
    n = row.shape[1]
    eye = iota((n, n), 0) == iota((n, n), 1)
    return jnp.sum(jnp.where(eye, row, 0.0), axis=1, keepdims=True)


def local(src, dst, sem):
    return pltpu.make_async_copy(src, dst, sem)


def send(src, dst, ssem, rsem, ep, tp):
    return pltpu.make_async_remote_copy(
        src_ref=src,
        dst_ref=dst,
        send_sem=ssem,
        recv_sem=rsem,
        device_id=(ep, tp),
        device_id_type=MESH,
    )


class Torus:
    def __init__(self, colour, ep, tp):
        y, x = lax.div(tp, SIDE), lax.rem(tp, SIDE)
        self.ep, self.tp, self.colour = ep, tp, colour
        self.a, self.b = (y, x) if colour == 0 else (x, y)

    def at(self, a, b):
        a, b = lax.rem(a + SIDE, SIDE), lax.rem(b + SIDE, SIDE)
        return a * SIDE + b if self.colour == 0 else b * SIDE + a


class Gather:
    def __init__(self, torus, buf, half, ssem, rsem):
        self.t, self.buf, self.ss, self.rs = torus, buf, ssem, rsem
        a, b = torus.a, torus.b
        self.am, self.ap = (lax.rem(a + k, SIDE) for k in (3, 1))
        self.bm, self.bp, self.bo = (lax.rem(b + k, SIDE) for k in (3, 1, 2))
        self.lo, self.hi = pl.ds(0, half), pl.ds(half, half)
        self.right_b, self.left_b = torus.at(a, b + 1), torus.at(a, b - 1)
        self.right_a, self.left_a = torus.at(a + 1, b), torus.at(a - 1, b)

    def put(self, block):
        self.buf[SIDE * self.t.a + self.t.b] = block

    def go(self, a, b, to, k, rows=slice(None)):
        src = self.buf.at[SIDE * a + b, rows]
        send(src, src, self.ss, self.rs.at[k], self.t.ep, to).start()

    def whole(self, n, k):
        d = self.buf.at[pl.ds(0, n)]
        return send(d, d, self.ss, self.rs.at[k], self.t.ep, self.t.tp)

    def got(self, k, n):
        self.whole(n, k).wait_recv()

    def stage(self, k):
        a, b = self.t.a, self.t.b
        if k == 0:
            self.go(a, b, self.right_b, 0)
            self.go(a, b, self.left_b, 0)
            self.go(a, b, self.right_a, 2)
            self.go(a, b, self.left_a, 2)
        elif k == 1:
            self.got(0, 2)
            self.go(a, self.bm, self.right_b, 1, self.lo)
            self.go(a, self.bp, self.left_b, 1, self.hi)
            for j in (self.bm, self.bp):
                self.go(a, j, self.right_a, 3)
                self.go(a, j, self.left_a, 3)
        elif k == 2:
            self.got(1, 1)
            self.go(a, self.bo, self.right_a, 4)
            self.go(a, self.bo, self.left_a, 4)
            self.got(2, 2)
            self.go(self.am, b, self.right_a, 5)
            self.got(3, 4)
            self.go(self.am, self.bm, self.right_a, 5)
            self.go(self.ap, self.bp, self.left_a, 5)
        elif k == 3:
            self.got(4, 2)
            self.go(self.ap, self.bo, self.left_a, 5)
        else:
            self.got(5, 4)
            self.whole(SIDE * SIDE - 1, 5).wait_send()


class Exchange:
    def __init__(self, ep, tp, n, cap, src, dst, ssem, rsem):
        self.ep, self.tp, self.n = ep, tp, n
        self.used = pl.ds(0, cap)
        self.src, self.dst, self.ss, self.rs = src, dst, ssem, rsem

    def start(self):
        self.dst[self.ep] = self.src[self.ep]

        def one(i, _):
            step = lax.select(lax.rem(i, 2) == 1, lax.div(i + 1, 2), self.n - lax.div(i, 2))
            peer = lax.rem(self.ep + step, self.n)
            send(
                self.src.at[peer, self.used],
                self.dst.at[self.ep, self.used],
                self.ss,
                self.rs,
                peer,
                self.tp,
            ).start()
            return 0

        lax.fori_loop(1, self.n, one, 0)

    def arrive(self):
        others = pl.ds(0, self.n - 1)
        d = send(
            self.src.at[others, self.used],
            self.dst.at[others, self.used],
            self.ss,
            self.rs,
            self.ep,
            self.tp,
        )
        d.wait_recv()
        d.wait_send()


def kernel(
    n_ep,
    n_tp,
    x_h,
    mix_gain_h,
    wq_h,
    wk_h,
    wv_h,
    q_gain_h,
    k_gain_h,
    gates_h,
    h_gain_h,
    wo_h,
    mx_h,
    moe_gain_h,
    routes_h,
    rweight_h,
    wg_h,
    wu_h,
    wd_h,
    mixer_out,
    moe_out,
    x,
    nx,
    wqkv,
    wo,
    mx,
    wgu,
    wd,
    kv,
    qa,
    acc,
    mx_run,
    hg0,
    hg1,
    sendb,
    recvb,
    retb,
    backb,
    onehot,
    g0,
    g1,
    h0,
    h1,
    wdn,
    mix_gain,
    q_gain,
    k_gain,
    gates,
    h_gain,
    moe_gain,
    routes,
    rweight,
    load_sem,
    near_recv,
    far_recv,
    kv_send,
    hg_s,
    hg_r,
    mg_s,
    mg_r,
    mh_s,
    mh_r,
    wd_s,
    wd_r,
    d_s,
    d_r,
    b_s,
    b_r,
):
    ep, tp = lax.axis_index("ep"), lax.axis_index("tp")
    z, core = lax.div(ep, 2), lax.rem(ep, 2)
    nz = n_ep // 2
    ups, dns = nz // 2, nz - 1 - nz // 2
    tq = x.shape[0]
    half_t = tq // 2
    fh = wd.shape[0]
    cap = 2 * g0.shape[1] // n_ep

    recvb[...] = jnp.zeros_like(recvb)
    backb[...] = jnp.zeros_like(backb)
    barrier = pltpu.get_barrier_semaphore()

    def greet_ep(i, _):
        pl.semaphore_signal(
            barrier, inc=1, device_id=(lax.rem(ep + i, n_ep), tp), device_id_type=MESH
        )
        return 0

    def greet_tp(i, _):
        pl.semaphore_signal(
            barrier, inc=1, device_id=(ep, lax.rem(tp + i, n_tp)), device_id_type=MESH
        )
        return 0

    lax.fori_loop(1, n_ep, greet_ep, 0)
    lax.fori_loop(1, n_tp, greet_tp, 0)

    loads = [
        local(s, d, load_sem.at[i])
        for i, (s, d) in enumerate(
            [
                (mx_h, mx),
                (moe_gain_h, moe_gain),
                (routes_h, routes),
                (x_h, x),
                (mix_gain_h, mix_gain),
                (wq_h, wqkv.at[pl.ds(0, HD)]),
                (wk_h, wqkv.at[pl.ds(HD, HD)]),
                (wv_h, wqkv.at[pl.ds(2 * HD, HD)]),
                (q_gain_h, q_gain),
                (k_gain_h, k_gain),
                (gates_h, gates),
                (wg_h.at[0], wgu.at[pl.ds(0, fh)]),
                (wu_h.at[0], wgu.at[pl.ds(fh, fh)]),
                (wd_h.at[0], wd),
                (wo_h, wo),
                (h_gain_h, h_gain),
                (rweight_h, rweight),
            ]
        )
    ]
    for d in loads:
        d.start()

    toks = mx.shape[0]
    slots = n_ep * SLOT
    for d in loads[0:3]:
        d.wait()
    r_rows = [routes[k : k + 1, :].astype(F32) for k in range(2)]
    experts = iota((n_ep, toks), 0).astype(F32)
    hot = [(experts == r).astype(F32) for r in r_rows]
    before = (iota((toks, toks), 0) < iota((toks, toks), 1)).astype(BF16)
    counts = dot((hot[0] + hot[1]).astype(BF16), before)
    for k in range(2):
        order = jnp.sum(hot[k] * counts, axis=0, keepdims=True)
        slot = (r_rows[k] * SLOT + order).astype(jnp.int32)
        onehot[k] = (iota((slots, toks), 0) == slot).astype(F32).astype(BF16)
    mxf = mx[...].astype(F32)
    mscale = lax.rsqrt(jnp.mean(mxf * mxf, axis=-1, keepdims=True) + EPS)
    cols = pl.ds(pl.multiple_of(tp * 128, 128), 128)
    mslice = (mx[:, cols].astype(F32) * mscale * moe_gain[:, cols]).astype(BF16)
    both = (onehot[0].astype(F32) + onehot[1].astype(F32)).astype(BF16)
    sendb[...] = dot(both, mslice).astype(BF16).reshape(n_ep, SLOT, 128)

    for d in loads[3:5]:
        d.wait()

    def norm_some(i, _):
        rows = pl.ds(pl.multiple_of(i * 64, 64), 64)
        nx[rows, :] = norm_rows(x[rows, :].astype(F32), mix_gain[...]).astype(BF16)
        return 0

    lax.fori_loop(0, tq // 64, norm_some, 0)
    for d in loads[5:11]:
        d.wait()
    qkv = dot(wqkv[...], nx[...], ((1,), (1,)))
    q = norm_cols(qkv[0:HD], to_col(q_gain[...])) * (HD**-0.5)
    k = norm_cols(qkv[HD : 2 * HD], to_col(k_gain[...]))
    qa[0:HD, :] = q.astype(BF16)
    ridx = iota((GR, tq), 0)
    qa[HD:KR, :] = jnp.where(ridx < 3, -1.0, 0.0).astype(BF16)
    g = gates[...]
    ghi = g.astype(BF16).astype(F32)
    gmid = (g - ghi).astype(BF16).astype(F32)
    glo = g - ghi - gmid
    grow = jnp.where(
        ridx == 0,
        ghi,
        jnp.where(ridx == 1, gmid, jnp.where(ridx == 2, glo, jnp.where(ridx == 3, 1.0, 0.0))),
    ).astype(BF16)
    kt, vt = k.astype(BF16), qkv[2 * HD :].astype(BF16)
    piece = tq // NCH
    for c in range(NCH):
        cc = slice(c * piece, (c + 1) * piece)
        kv[ep, c, 0:HD, :] = kt[:, cc]
        kv[ep, c, HD:KR, :] = grow[:, cc]
        kv[ep, c, KR:BR, :] = vt[:, cc]

    pl.semaphore_wait(barrier, n_ep - 1 + n_tp - 1)

    dispatch = Exchange(ep, tp, n_ep, cap, sendb, recvb, d_s, d_r)
    dispatch.start()

    def features(t):
        return wd.at[:, pl.ds(pl.multiple_of(t * 128, 128), 128)]

    def give_weights(i, _):
        peer = lax.rem(tp + i, n_tp)
        send(features(peer), wdn.at[tp], wd_s, wd_r, ep, peer).start()
        return 0

    def take_weights():
        others = wdn.at[pl.ds(0, n_tp - 1)]
        w = send(others, others, wd_s, wd_r, ep, tp)
        w.wait_recv()
        w.wait_send()

    def hop(slot, c, to_ep):
        piece_ref, sem = kv.at[slot, c], near_recv.at[lax.div(slot, 2), c]
        return send(piece_ref, piece_ref, kv_send, sem, to_ep, tp)

    def hand(slot, c):
        piece_ref, sem = kv.at[slot, c], far_recv.at[lax.div(slot, 2)]
        return send(piece_ref, piece_ref, kv_send, sem, sib_ep, tp)

    up_ep = lax.rem(z + 1, nz) * 2 + core
    dn_ep = lax.rem(z + nz - 1, nz) * 2 + core
    sib_ep = z * 2 + 1 - core

    def slot_of(step, whose):
        return lax.rem(z + step + nz, nz) * 2 + whose

    for c in range(NCH):
        hop(ep, c, up_ep).start()
        hop(ep, c, dn_ep).start()
        hand(ep, c).start()

    def flash(slots_in, diagonal=False):
        top, got = (None, None) if diagonal else (mx_run[...], acc[...])
        halves = [
            [jnp.concatenate([kv[i, h * NH + c] for c in range(NH)], axis=1) for h in range(2)]
            for i in slots_in
        ]
        scores = [[dot(p[0:KR], qa[...], ((0,), (0,))) for p in pair] for pair in halves]
        for pair, s in zip(halves, scores):
            if diagonal:
                s = [
                    jnp.where(
                        iota((half_t, tq), 0) + h * half_t <= iota((half_t, tq), 1), s[h], -1e30
                    )
                    for h in range(2)
                ]
            new = jnp.maximum(
                jnp.max(s[0], axis=0, keepdims=True), jnp.max(s[1], axis=0, keepdims=True)
            )
            if top is not None:
                new = jnp.maximum(top, new)
                got = got * jnp.exp(top - new)
            w = [jnp.exp(p - new).astype(BF16) for p in s]
            o = dot(
                jnp.concatenate([p[HD:] for p in pair], axis=1), jnp.concatenate(w, axis=0)
            )
            got = o if got is None else got + o
            top = new
        acc[...] = got
        mx_run[...] = top

    loads[13].wait()
    lax.fori_loop(1, n_tp, give_weights, 0)
    wdn[tp] = wd[:, pl.ds(pl.multiple_of(tp * 128, 128), 128)]
    flash([ep], diagonal=True)

    def take(one, other):
        @pl.when(jnp.maximum(one, other) < ep)
        def _():
            flash([one, other])

        @pl.when(jnp.logical_and(jnp.minimum(one, other) < ep, jnp.maximum(one, other) >= ep))
        def _():
            flash([jnp.minimum(one, other)])

    def wait_piece(slot, c):
        hop(slot, c, up_ep).wait_recv()

    def wait_block(slot):
        sem = far_recv.at[lax.div(slot, 2)]
        send(kv.at[slot], kv.at[slot], kv_send, sem, sib_ep, tp).wait_recv()

    t0, t1 = Torus(0, ep, tp), Torus(1, ep, tp)
    rows = g0.shape[1]
    mg = [
        Gather(t0, g0, rows // 2, mg_s.at[0], mg_r.at[0]),
        Gather(t1, g1, rows // 2, mg_s.at[1], mg_r.at[1]),
    ]
    mh = [
        Gather(t0, h0, fh // 4, mh_s.at[0], mh_r.at[0]),
        Gather(t1, h1, fh // 4, mh_s.at[1], mh_r.at[1]),
    ]
    tiles = range(SIDE * SIDE)
    places = [list(tiles), [SIDE * (t % SIDE) + t // SIDE for t in tiles]]
    returns = Exchange(ep, tp, n_ep, cap, retb, backb, b_s, b_r)

    def pick(rows_out, rows_in, wide_first):
        wide, dense = (0, 1) if wide_first else (1, 0)
        w, d = iota((rows_out, rows_in), wide), iota((rows_out, rows_in), dense)
        i = lax.rem(w, SLOT)
        hit = jnp.logical_and(lax.div(w, SLOT) * cap + i == d, i < cap)
        return hit.astype(F32).astype(BF16)

    def pack_rows():
        dispatch.arrive()
        packed = dot(
            pick(2 * rows, slots, False), recvb[...].reshape(slots, 128)
        ).astype(BF16)
        mg[0].put(packed[:rows])
        mg[1].put(packed[rows:])
        for m in mg:
            m.stage(0)

    def experts_now():
        for d in loads[11:13]:
            d.wait()
        for m in mg:
            m.stage(4)
        wide = jnp.concatenate(
            [
                jnp.concatenate([buf[i] for i in place], axis=1)
                for buf, place in zip((g0, g1), places)
            ],
            axis=0,
        )
        sums = dot(wgu[...], wide, ((1,), (1,)))
        gs, us = sums[:fh], sums[fh:]
        hidden = (gs / (1.0 + jnp.exp(-gs)) * us).astype(BF16)
        mh[0].put(hidden[: fh // 2])
        mh[1].put(hidden[fh // 2 :])
        for m in mh:
            m.stage(0)

    def give_back():
        take_weights()
        for m in mh:
            m.stage(4)
        tall = jnp.concatenate(
            [
                buf[i] for both in zip(*places) for buf, i in zip((h0, h1), both)
            ],
            axis=0,
        )
        rows_out = dot(wdn[...].reshape(n_tp * fh, 128), tall, ((0,), (0,))).astype(BF16)
        retb[...] = (
            dot(pick(slots, 2 * rows, True), rows_out, ((1,), (1,)))
            .astype(BF16)
            .reshape(n_ep, SLOT, 128)
        )
        returns.start()

    hooks = {
        (1, 0): pack_rows,
        (2, 0): lambda: [m.stage(1) for m in mg],
        (3, 0): lambda: [m.stage(2) for m in mg],
        (4, 1): lambda: [m.stage(3) for m in mg],
        (5, 1): experts_now,
        (6, 2): lambda: [m.stage(1) for m in mh],
        (7, 2): lambda: [m.stage(2) for m in mh],
        (8, 2): lambda: [m.stage(3) for m in mh],
    }

    def run_hooks(s, part):
        for (at, which), hook in hooks.items():
            if which == part:

                @pl.when(s == at)
                def _():
                    hook()

    def ring(s, _):
        up, dn = slot_of(-s, core), slot_of(s, core)
        for c in range(NCH):
            wait_piece(up, c)

            @pl.when(s < ups)
            def _():
                hop(up, c, up_ep).start()

            hand(up, c).start()

            @pl.when(s <= dns)
            def _():
                wait_piece(dn, c)

                @pl.when(s < dns)
                def _():
                    hop(dn, c, dn_ep).start()

                hand(dn, c).start()

            if c == 1:
                ring_up, ring_dn = slot_of(1 - s, core), slot_of(s - 1, core)
                take(*(lax.select(s >= 2, i, n_ep) for i in (ring_up, ring_dn)))
            elif c == 3:
                far_up, far_dn = slot_of(1 - s, 1 - core), slot_of(s - 1, 1 - core)
                wait_block(far_up)

                @pl.when(s >= 2)
                def _():
                    wait_block(far_dn)

                take(far_up, lax.select(s >= 2, far_dn, n_ep))
            run_hooks(s, c)
        return 0

    lax.fori_loop(1, ups + 1, ring, 0)
    last = slot_of(-ups, 1 - core)
    wait_block(last)
    take(slot_of(-ups, core), last)

    loads[15].wait()
    att = acc[GR:, :] / acc[3:4, :]
    head = norm_cols(att, to_col(h_gain[...])).astype(BF16)
    hg = [
        Gather(t0, hg0, HD // 2, hg_s.at[0], hg_r.at[0]),
        Gather(t1, hg1, HD // 2, hg_s.at[1], hg_r.at[1]),
    ]
    for i, m in enumerate(hg):
        m.put(head[:, i * half_t : (i + 1) * half_t])
        m.stage(0)
    for m in hg:
        m.stage(1)
    give_back()
    for m in hg:
        m.stage(2)
    for m in hg:
        m.stage(3)
    loads[14].wait()
    loads[16].wait()
    for i, (m, buf) in enumerate(((hg[0], hg0), (hg[1], hg1))):
        m.stage(4)
        tall = jnp.concatenate([buf[j] for j in places[i]], axis=0)
        o = dot(tall, wo[...], ((0,), (0,)))
        mixer_out[i * half_t : (i + 1) * half_t, :] = o.astype(BF16)

    returns.arrive()
    back = backb[...].reshape(slots, 128)
    total = None
    for k in range(2):
        got = dot(onehot[k], back, ((0,), (0,))) * to_col(rweight[k : k + 1, :])
        total = got if total is None else total + got
    moe_out[...] = total.astype(BF16)

    most = kv.at[pl.ds(0, n_ep - 1)]
    send(most, most, kv_send, far_recv.at[z], sib_ep, tp).wait_send()


def body(
    n_ep,
    n_tp,
    attn_in,
    mix_gain,
    query_weight,
    key_weight,
    value_weight,
    query_gain,
    key_gain,
    log_cache,
    head_gain,
    out_weight,
    moe_in,
    moe_gain,
    routes,
    route_weight,
    expert_gate,
    expert_up,
    expert_down,
):
    tq, d = attn_in.shape
    toks = moe_in.shape[0]
    fh = expert_down.shape[1]
    cap = 3 * toks * routes.shape[1] // (2 * n_ep)
    rows = n_ep * cap // 2
    vm = pl.BlockSpec(memory_space=pltpu.VMEM)
    hbm = pl.BlockSpec(memory_space=pl.ANY)
    dma = pltpu.SemaphoreType.DMA

    def v(*shape, dtype=BF16):
        return pltpu.VMEM(shape, dtype)

    nz = n_ep // 2
    scratch = [
        v(tq, d),
        v(tq, d),
        v(3 * HD, d),
        v(n_tp * HD, 128),
        v(toks, d),
        v(2 * fh, d),
        v(fh, d),
        v(n_ep, NCH, BR, tq // NCH),
        v(KR, tq),
        v(GR + HD, tq, dtype=F32),
        v(1, tq, dtype=F32),
        v(n_tp, HD, tq // 2),
        v(n_tp, HD, tq // 2),
        v(n_ep, SLOT, 128),
        v(n_ep, SLOT, 128),
        v(n_ep, SLOT, 128),
        v(n_ep, SLOT, 128),
        v(2, n_ep * SLOT, toks),
        v(n_tp, rows, 128),
        v(n_tp, rows, 128),
        v(n_tp, fh // 2, 2 * rows),
        v(n_tp, fh // 2, 2 * rows),
        v(n_tp, fh, 128),
        v(1, d, dtype=F32),
        v(1, HD, dtype=F32),
        v(1, HD, dtype=F32),
        v(1, tq, dtype=F32),
        v(1, HD, dtype=F32),
        v(1, d, dtype=F32),
        v(2, toks, dtype=jnp.int32),
        v(2, toks, dtype=F32),
        dma((17,)),
        dma((nz, NCH)),
        dma((nz,)),
        dma,
        dma((2,)),
        dma((2, 6)),
        dma((2,)),
        dma((2, 6)),
        dma((2,)),
        dma((2, 6)),
        dma,
        dma,
        dma,
        dma,
        dma,
        dma,
    ]
    return pl.pallas_call(
        functools.partial(kernel, n_ep, n_tp),
        out_shape=(
            jax.ShapeDtypeStruct((tq, 128), BF16),
            jax.ShapeDtypeStruct((toks, 128), BF16),
        ),
        in_specs=[hbm] * 17,
        out_specs=(vm, vm),
        scratch_shapes=scratch,
        compiler_params=pltpu.CompilerParams(
            collective_id=0, has_side_effects=True, vmem_limit_bytes=60 * 1024 * 1024
        ),
    )(
        attn_in,
        mix_gain.reshape(1, -1),
        query_weight.T,
        key_weight.T,
        value_weight.T,
        query_gain.reshape(1, -1),
        key_gain.reshape(1, -1),
        log_cache.reshape(1, -1),
        head_gain.reshape(1, -1),
        out_weight,
        moe_in,
        moe_gain.reshape(1, -1),
        routes.T,
        route_weight.T,
        jnp.swapaxes(expert_gate, 1, 2),
        jnp.swapaxes(expert_up, 1, 2),
        expert_down,
    )


def solution(mesh):
    n_ep, n_tp = mesh.shape["ep"], mesh.shape["tp"]
    in_specs = (
        P("ep", None),
        P(),
        P(None, "tp"),
        P(None, "tp"),
        P(None, "tp"),
        P(),
        P(),
        P("ep", "tp"),
        P("tp"),
        P(None, "tp"),
        P("ep", None),
        P(),
        P("ep", None),
        P("ep", None),
        P("ep", None, "tp"),
        P("ep", None, "tp"),
        P("ep", "tp", None),
    )
    out_specs = (P("ep", "tp"), P("ep", "tp"))
    return jax.shard_map(
        functools.partial(body, n_ep, n_tp),
        mesh=mesh,
        in_specs=in_specs,
        out_specs=out_specs,
        check_vma=False,
    )
```

```python
import functools

import jax
import jax.numpy as jnp
from jax import lax
from jax.experimental import pallas as pl
from jax.experimental.pallas import tpu as pltpu
from jax.sharding import PartitionSpec as P

HD = 64
EPS = 1e-06
GR = 8
KR = HD + GR
BR = KR + HD
SIDE = 4
SLOT = 16
NCH = 4
NH = NCH // 2
DISPATCH_AFTER = 0
MESH = pl.DeviceIdType.MESH
F32 = jnp.float32
BF16 = jnp.bfloat16


def dot(a, b, dims=((1,), (0,))):
    return lax.dot_general(a, b, (dims, ((), ())), preferred_element_type=F32)


def iota(shape, dim):
    return lax.broadcasted_iota(jnp.int32, shape, dim)


def norm_rows(x, gain):
    return x * lax.rsqrt(jnp.mean(x * x, axis=-1, keepdims=True) + EPS) * gain


def norm_cols(x, gain):
    return x * lax.rsqrt(jnp.mean(x * x, axis=0, keepdims=True) + EPS) * gain


def to_col(row):
    n = row.shape[1]
    eye = iota((n, n), 0) == iota((n, n), 1)
    return jnp.sum(jnp.where(eye, row, 0.0), axis=1, keepdims=True)


def local(src, dst, sem):
    return pltpu.make_async_copy(src, dst, sem)


def send(src, dst, ssem, rsem, ep, tp):
    return pltpu.make_async_remote_copy(
        src_ref=src,
        dst_ref=dst,
        send_sem=ssem,
        recv_sem=rsem,
        device_id=(ep, tp),
        device_id_type=MESH,
    )


class Torus:
    def __init__(self, colour, ep, tp):
        y, x = lax.div(tp, SIDE), lax.rem(tp, SIDE)
        self.ep, self.tp, self.colour = ep, tp, colour
        self.a, self.b = (y, x) if colour == 0 else (x, y)

    def at(self, a, b):
        a, b = lax.rem(a + SIDE, SIDE), lax.rem(b + SIDE, SIDE)
        return a * SIDE + b if self.colour == 0 else b * SIDE + a


class Gather:
    def __init__(self, torus, buf, half, ssem, rsem):
        self.t, self.buf, self.ss, self.rs = torus, buf, ssem, rsem
        a, b = torus.a, torus.b
        self.am, self.ap = (lax.rem(a + k, SIDE) for k in (3, 1))
        self.bm, self.bp, self.bo = (lax.rem(b + k, SIDE) for k in (3, 1, 2))
        self.lo, self.hi = pl.ds(0, half), pl.ds(half, half)
        self.right_b, self.left_b = torus.at(a, b + 1), torus.at(a, b - 1)
        self.right_a, self.left_a = torus.at(a + 1, b), torus.at(a - 1, b)

    def put(self, block):
        self.buf[SIDE * self.t.a + self.t.b] = block

    def go(self, a, b, to, k, rows=slice(None)):
        src = self.buf.at[SIDE * a + b, rows]
        send(src, src, self.ss, self.rs.at[k], self.t.ep, to).start()

    def whole(self, n, k):
        d = self.buf.at[pl.ds(0, n)]
        return send(d, d, self.ss, self.rs.at[k], self.t.ep, self.t.tp)

    def got(self, k, n):
        self.whole(n, k).wait_recv()

    def stage(self, k):
        a, b = self.t.a, self.t.b
        if k == 0:
            self.go(a, b, self.right_b, 0)
            self.go(a, b, self.left_b, 0)
        elif k == 1:
            self.got(0, 2)
            self.go(a, self.bm, self.right_b, 1, self.lo)
            self.go(a, self.bp, self.left_b, 1, self.hi)
        elif k == 2:
            self.got(1, 1)
            self.go(a, self.bo, self.right_a, 4)
            self.go(a, self.bo, self.left_a, 4)
            self.got(2, 2)
            self.go(self.am, b, self.right_a, 5)
            self.got(3, 4)
            self.go(self.am, self.bm, self.right_a, 5)
            self.go(self.ap, self.bp, self.left_a, 5)
        elif k == 3:
            self.got(4, 2)
            self.go(self.ap, self.bo, self.left_a, 5)
        else:
            self.got(5, 4)
            self.whole(SIDE * SIDE - 1, 5).wait_send()

    def across(self, k):
        a, b = self.t.a, self.t.b
        if k == 0:
            self.go(a, b, self.right_a, 2)
            self.go(a, b, self.left_a, 2)
        elif k == 1:
            for j in (self.bm, self.bp):
                self.go(a, j, self.right_a, 3)
                self.go(a, j, self.left_a, 3)


def step_all(gathers, k):
    for m in gathers:
        m.stage(k)
    for m in gathers:
        m.across(k)


class Exchange:
    def __init__(self, ep, tp, n, cap, src, dst, ssem, rsem):
        self.ep, self.tp, self.n = ep, tp, n
        self.used = pl.ds(0, cap)
        self.src, self.dst, self.ss, self.rs = src, dst, ssem, rsem

    def start(self):
        self.dst[self.ep] = self.src[self.ep]

        def one(i, _):
            step = lax.select(lax.rem(i, 2) == 1, lax.div(i + 1, 2), self.n - lax.div(i, 2))
            peer = lax.rem(self.ep + step, self.n)
            send(
                self.src.at[peer, self.used],
                self.dst.at[self.ep, self.used],
                self.ss,
                self.rs,
                peer,
                self.tp,
            ).start()
            return 0

        lax.fori_loop(1, self.n, one, 0)

    def arrive(self):
        others = pl.ds(0, self.n - 1)
        d = send(
            self.src.at[others, self.used],
            self.dst.at[others, self.used],
            self.ss,
            self.rs,
            self.ep,
            self.tp,
        )
        d.wait_recv()
        d.wait_send()


def kernel(
    n_ep,
    n_tp,
    x_h,
    mix_gain_h,
    wq_h,
    wk_h,
    wv_h,
    q_gain_h,
    k_gain_h,
    gates_h,
    h_gain_h,
    wo_h,
    mx_h,
    moe_gain_h,
    routes_h,
    rweight_h,
    wg_h,
    wu_h,
    wd_h,
    mixer_out,
    moe_out,
    x,
    nx,
    wqkv,
    wo,
    wot,
    wdt,
    to_dense,
    to_wide,
    mx,
    wgu,
    wd,
    kv,
    qa,
    acc,
    mx_run,
    hg0,
    hg1,
    sendb,
    recvb,
    retb,
    backb,
    onehot,
    g0,
    g1,
    h0,
    h1,
    wdn,
    mix_gain,
    q_gain,
    k_gain,
    gates,
    h_gain,
    moe_gain,
    routes,
    rweight,
    load_sem,
    near_recv,
    far_recv,
    kv_send,
    hg_s,
    hg_r,
    mg_s,
    mg_r,
    mh_s,
    mh_r,
    wd_s,
    wd_r,
    d_s,
    d_r,
    b_s,
    b_r,
):
    ep, tp = lax.axis_index("ep"), lax.axis_index("tp")
    z, core = lax.div(ep, 2), lax.rem(ep, 2)
    nz = n_ep // 2
    ups, dns = nz // 2, nz - 1 - nz // 2
    tq = x.shape[0]
    half_t = tq // 2
    fh = wd.shape[0]
    cap = 2 * g0.shape[1] // n_ep

    barrier = pltpu.get_barrier_semaphore()

    def far_first(i):
        return n_ep // 2 + lax.select(lax.rem(i, 2) == 1, lax.div(i, 2), -lax.div(i, 2))

    def greet_ep(i, _):
        pl.semaphore_signal(
            barrier, inc=1, device_id=(lax.rem(ep + far_first(i), n_ep), tp), device_id_type=MESH
        )
        return 0

    def greet_tp(i, _):
        pl.semaphore_signal(
            barrier, inc=1, device_id=(ep, lax.rem(tp + i, n_tp)), device_id_type=MESH
        )
        return 0

    lax.fori_loop(1, n_ep, greet_ep, 0)
    lax.fori_loop(1, n_tp, greet_tp, 0)

    loads = [
        local(s, d, load_sem.at[i])
        for i, (s, d) in enumerate(
            [
                (mx_h, mx),
                (moe_gain_h, moe_gain),
                (routes_h, routes),
                (x_h, x),
                (mix_gain_h, mix_gain),
                (wq_h, wqkv.at[pl.ds(0, HD)]),
                (wk_h, wqkv.at[pl.ds(HD, HD)]),
                (wv_h, wqkv.at[pl.ds(2 * HD, HD)]),
                (q_gain_h, q_gain),
                (k_gain_h, k_gain),
                (gates_h, gates),
                (wg_h.at[0], wgu.at[pl.ds(0, fh)]),
                (wu_h.at[0], wgu.at[pl.ds(fh, fh)]),
                (wd_h.at[0], wd),
                (wo_h, wo),
                (h_gain_h, h_gain),
                (rweight_h, rweight),
            ]
        )
    ]
    for d in loads:
        d.start()

    toks = mx.shape[0]
    slots = n_ep * SLOT
    for d in loads[0:3]:
        d.wait()
    r_rows = [routes[k : k + 1, :].astype(F32) for k in range(2)]
    experts = iota((n_ep, toks), 0).astype(F32)
    hot = [(experts == r).astype(F32) for r in r_rows]
    before = (iota((toks, toks), 0) < iota((toks, toks), 1)).astype(BF16)
    counts = dot((hot[0] + hot[1]).astype(BF16), before)
    for k in range(2):
        order = jnp.sum(hot[k] * counts, axis=0, keepdims=True)
        slot = (r_rows[k] * SLOT + order).astype(jnp.int32)
        onehot[k] = (iota((slots, toks), 0) == slot).astype(F32).astype(BF16)
    mxf = mx[...].astype(F32)
    mscale = lax.rsqrt(jnp.mean(mxf * mxf, axis=-1, keepdims=True) + EPS)
    cols = pl.ds(pl.multiple_of(tp * 128, 128), 128)
    mslice = (mx[:, cols].astype(F32) * mscale * moe_gain[:, cols]).astype(BF16)
    both = (onehot[0].astype(F32) + onehot[1].astype(F32)).astype(BF16)
    sendb[...] = dot(both, mslice).astype(BF16).reshape(n_ep, SLOT, 128)

    for d in loads[3:5]:
        d.wait()

    def norm_some(i, _):
        rows = pl.ds(pl.multiple_of(i * 64, 64), 64)
        nx[rows, :] = norm_rows(x[rows, :].astype(F32), mix_gain[...]).astype(BF16)
        return 0

    lax.fori_loop(0, tq // 64, norm_some, 0)
    for d in loads[5:11]:
        d.wait()
    qkv = dot(wqkv[...], nx[...], ((1,), (1,)))
    q = norm_cols(qkv[0:HD], to_col(q_gain[...])) * (HD**-0.5)
    k = norm_cols(qkv[HD : 2 * HD], to_col(k_gain[...]))
    qa[0:HD, :] = q.astype(BF16)
    ridx = iota((GR, tq), 0)
    qa[HD:KR, :] = jnp.where(ridx < 3, -1.0, 0.0).astype(BF16)
    g = gates[...]
    ghi = g.astype(BF16).astype(F32)
    gmid = (g - ghi).astype(BF16).astype(F32)
    glo = g - ghi - gmid
    grow = jnp.where(
        ridx == 0,
        ghi,
        jnp.where(ridx == 1, gmid, jnp.where(ridx == 2, glo, jnp.where(ridx == 3, 1.0, 0.0))),
    ).astype(BF16)
    kt, vt = k.astype(BF16), qkv[2 * HD :].astype(BF16)
    piece = tq // NCH
    for c in range(NCH):
        cc = slice(c * piece, (c + 1) * piece)
        kv[ep, c, 0:HD, :] = kt[:, cc]
        kv[ep, c, HD:KR, :] = grow[:, cc]
        kv[ep, c, KR:BR, :] = vt[:, cc]

    def pick(rows_out, rows_in, wide_first):
        wide, dense = (0, 1) if wide_first else (1, 0)
        w, d = iota((rows_out, rows_in), wide), iota((rows_out, rows_in), dense)
        i = lax.rem(w, SLOT)
        hit = jnp.logical_and(lax.div(w, SLOT) * cap + i == d, i < cap)
        return hit.astype(F32).astype(BF16)

    to_dense[...] = pick(2 * g0.shape[1], slots, False)
    to_wide[...] = pick(slots, 2 * g0.shape[1], True)
    loads[14].wait()
    wot[...] = wo[...].astype(F32).T.astype(BF16)
    pl.semaphore_wait(barrier, n_ep - 1 + n_tp - 1)

    dispatch = Exchange(ep, tp, n_ep, cap, sendb, recvb, d_s, d_r)

    def features(t):
        return wd.at[:, pl.ds(pl.multiple_of(t * 128, 128), 128)]

    def give_weights(i, _):
        peer = lax.rem(tp + i, n_tp)
        send(features(peer), wdn.at[tp], wd_s, wd_r, ep, peer).start()
        return 0

    def take_weights():
        others = wdn.at[pl.ds(0, n_tp - 1)]
        w = send(others, others, wd_s, wd_r, ep, tp)
        w.wait_recv()
        w.wait_send()

    def hop(slot, c, to_ep):
        piece_ref, sem = kv.at[slot, c], near_recv.at[lax.div(slot, 2), c]
        return send(piece_ref, piece_ref, kv_send, sem, to_ep, tp)

    def hand(slot, c):
        piece_ref, sem = kv.at[slot, c], far_recv.at[lax.div(slot, 2)]
        return send(piece_ref, piece_ref, kv_send, sem, sib_ep, tp)

    up_ep = lax.rem(z + 1, nz) * 2 + core
    dn_ep = lax.rem(z + nz - 1, nz) * 2 + core
    sib_ep = z * 2 + 1 - core

    def slot_of(step, whose):
        return lax.rem(z + step + nz, nz) * 2 + whose

    for c in range(NCH):
        hop(ep, c, up_ep).start()
        hop(ep, c, dn_ep).start()
        hand(ep, c).start()
        if c == DISPATCH_AFTER:
            dispatch.start()

    def flash(slots_in, diagonal=False):
        top, got = (None, None) if diagonal else (mx_run[...], acc[...])
        halves = [
            [jnp.concatenate([kv[i, h * NH + c] for c in range(NH)], axis=1) for h in range(2)]
            for i in slots_in
        ]
        scores = [[dot(p[0:KR], qa[...], ((0,), (0,))) for p in pair] for pair in halves]
        for pair, s in zip(halves, scores):
            if diagonal:
                s = [
                    jnp.where(
                        iota((half_t, tq), 0) + h * half_t <= iota((half_t, tq), 1), s[h], -1e30
                    )
                    for h in range(2)
                ]
            new = jnp.maximum(
                jnp.max(s[0], axis=0, keepdims=True), jnp.max(s[1], axis=0, keepdims=True)
            )
            if top is not None:
                new = jnp.maximum(top, new)
                got = got * jnp.exp(top - new)
            w = [jnp.exp(p - new).astype(BF16) for p in s]
            o = dot(
                jnp.concatenate([p[HD:] for p in pair], axis=1), jnp.concatenate(w, axis=0)
            )
            got = o if got is None else got + o
            top = new
        acc[...] = got
        mx_run[...] = top

    loads[13].wait()
    lax.fori_loop(1, n_tp, give_weights, 0)
    wdn[tp] = wd[:, pl.ds(pl.multiple_of(tp * 128, 128), 128)]
    flash([ep], diagonal=True)

    def take(one, other):
        @pl.when(jnp.maximum(one, other) < ep)
        def _():
            flash([one, other])

        @pl.when(jnp.logical_and(jnp.minimum(one, other) < ep, jnp.maximum(one, other) >= ep))
        def _():
            flash([jnp.minimum(one, other)])

    def wait_piece(slot, c):
        hop(slot, c, up_ep).wait_recv()

    def wait_block(slot):
        sem = far_recv.at[lax.div(slot, 2)]
        send(kv.at[slot], kv.at[slot], kv_send, sem, sib_ep, tp).wait_recv()

    t0, t1 = Torus(0, ep, tp), Torus(1, ep, tp)
    rows = g0.shape[1]
    mg = [
        Gather(t0, g0, rows // 2, mg_s.at[0], mg_r.at[0]),
        Gather(t1, g1, rows // 2, mg_s.at[1], mg_r.at[1]),
    ]
    mh = [
        Gather(t0, h0, fh // 4, mh_s.at[0], mh_r.at[0]),
        Gather(t1, h1, fh // 4, mh_s.at[1], mh_r.at[1]),
    ]
    tiles = range(SIDE * SIDE)
    places = [list(tiles), [SIDE * (t % SIDE) + t // SIDE for t in tiles]]
    returns = Exchange(ep, tp, n_ep, cap, retb, backb, b_s, b_r)

    def filled(buf):
        used = iota((n_ep, SLOT, 128), 1) < cap
        return jnp.where(used, buf[...].astype(F32), 0.0).astype(BF16).reshape(slots, 128)

    def pack_rows():
        dispatch.arrive()
        packed = dot(
            to_dense[...], filled(recvb)
        ).astype(BF16)
        mg[0].put(packed[:rows])
        mg[1].put(packed[rows:])
        step_all(mg, 0)

    def experts_now():
        for d in loads[11:13]:
            d.wait()
        take_weights()
        wdt[...] = wdn[...].reshape(n_tp * fh, 128).astype(F32).T.astype(BF16)
        step_all(mg, 4)
        wide = jnp.concatenate(
            [
                jnp.concatenate([buf[i] for i in place], axis=1)
                for buf, place in zip((g0, g1), places)
            ],
            axis=0,
        )
        sums = dot(wgu[...], wide, ((1,), (1,)))
        gs, us = sums[:fh], sums[fh:]
        hidden = (gs / (1.0 + jnp.exp(-gs)) * us).astype(BF16)
        mh[0].put(hidden[: fh // 2])
        mh[1].put(hidden[fh // 2 :])
        step_all(mh, 0)

    def give_back():
        step_all(mh, 4)
        tall = jnp.concatenate(
            [
                buf[i] for both in zip(*places) for buf, i in zip((h0, h1), both)
            ],
            axis=0,
        )
        rows_out = dot(wdt[...], tall).astype(BF16)
        retb[...] = (
            dot(to_wide[...], rows_out, ((1,), (1,)))
            .astype(BF16)
            .reshape(n_ep, SLOT, 128)
        )
        returns.start()

    hooks = {
        (1, 3): pack_rows,
        (2, 3): lambda: step_all(mg, 1),
        (4, 0): lambda: step_all(mg, 2),
        (5, 0): lambda: step_all(mg, 3),
        (6, 0): experts_now,
        (7, 0): lambda: step_all(mh, 1),
        (8, 0): lambda: step_all(mh, 2),
        (9, 0): lambda: step_all(mh, 3),
    }

    def run_hooks(s, part):
        for (at, which), hook in hooks.items():
            if which == part and at <= ups:

                @pl.when(s == at)
                def _():
                    hook()

    def ring(s, _):
        up, dn = slot_of(-s, core), slot_of(s, core)
        for c in range(NCH):
            wait_piece(up, c)

            @pl.when(s < (ups if c < NH else dns))
            def _():
                hop(up, c, up_ep).start()

            hand(up, c).start()

            @pl.when(s <= dns)
            def _():
                wait_piece(dn, c)

                @pl.when(s < (dns if c < NH else ups))
                def _():
                    hop(dn, c, dn_ep).start()

                hand(dn, c).start()

            if c == 1:
                ring_up, ring_dn = slot_of(1 - s, core), slot_of(s - 1, core)
                take(*(lax.select(s >= 2, i, n_ep) for i in (ring_up, ring_dn)))
            elif c == 3:
                far_up, far_dn = slot_of(1 - s, 1 - core), slot_of(s - 1, 1 - core)
                wait_block(far_up)

                @pl.when(s >= 2)
                def _():
                    wait_block(far_dn)

                take(far_up, lax.select(s >= 2, far_dn, n_ep))
            run_hooks(s, c)
        return 0

    lax.fori_loop(1, ups + 1, ring, 0)
    last = slot_of(-ups, 1 - core)
    wait_block(last)
    take(slot_of(-ups, core), last)

    loads[15].wait()
    att = acc[GR:, :] / acc[3:4, :]
    head = norm_cols(att, to_col(h_gain[...])).astype(BF16)
    hg = [
        Gather(t0, hg0, HD // 2, hg_s.at[0], hg_r.at[0]),
        Gather(t1, hg1, HD // 2, hg_s.at[1], hg_r.at[1]),
    ]
    for i, m in enumerate(hg):
        m.put(head[:, i * half_t : (i + 1) * half_t])
    step_all(hg, 0)
    for (at, _), hook in hooks.items():
        if at == ups + 1:
            hook()
    step_all(hg, 1)
    give_back()
    for (at, _), hook in hooks.items():
        if at == ups + 2:
            hook()
    step_all(hg, 2)
    step_all(hg, 3)
    loads[16].wait()
    for i, (m, buf) in enumerate(((hg[0], hg0), (hg[1], hg1))):
        m.stage(4)
        tall = jnp.concatenate([buf[j] for j in places[i]], axis=0)
        o = dot(wot[...], tall)
        mixer_out[i * half_t : (i + 1) * half_t, :] = o.T.astype(BF16)

    returns.arrive()
    back = filled(backb)
    total = None
    for k in range(2):
        got = dot(onehot[k], back, ((0,), (0,))) * to_col(rweight[k : k + 1, :])
        total = got if total is None else total + got
    moe_out[...] = total.astype(BF16)

    most = kv.at[pl.ds(0, n_ep - 1)]
    send(most, most, kv_send, far_recv.at[z], sib_ep, tp).wait_send()


def body(
    n_ep,
    n_tp,
    attn_in,
    mix_gain,
    query_weight,
    key_weight,
    value_weight,
    query_gain,
    key_gain,
    log_cache,
    head_gain,
    out_weight,
    moe_in,
    moe_gain,
    routes,
    route_weight,
    expert_gate,
    expert_up,
    expert_down,
):
    tq, d = attn_in.shape
    toks = moe_in.shape[0]
    fh = expert_down.shape[1]
    cap = 3 * toks * routes.shape[1] // (2 * n_ep)
    rows = n_ep * cap // 2
    vm = pl.BlockSpec(memory_space=pltpu.VMEM)
    hbm = pl.BlockSpec(memory_space=pl.ANY)
    dma = pltpu.SemaphoreType.DMA

    def v(*shape, dtype=BF16):
        return pltpu.VMEM(shape, dtype)

    nz = n_ep // 2
    scratch = [
        v(tq, d),
        v(tq, d),
        v(3 * HD, d),
        v(n_tp * HD, 128),
        v(128, n_tp * HD),
        v(128, n_tp * fh),
        v(2 * rows, n_ep * SLOT),
        v(n_ep * SLOT, 2 * rows),
        v(toks, d),
        v(2 * fh, d),
        v(fh, d),
        v(n_ep, NCH, BR, tq // NCH),
        v(KR, tq),
        v(GR + HD, tq, dtype=F32),
        v(1, tq, dtype=F32),
        v(n_tp, HD, tq // 2),
        v(n_tp, HD, tq // 2),
        v(n_ep, SLOT, 128),
        v(n_ep, SLOT, 128),
        v(n_ep, SLOT, 128),
        v(n_ep, SLOT, 128),
        v(2, n_ep * SLOT, toks),
        v(n_tp, rows, 128),
        v(n_tp, rows, 128),
        v(n_tp, fh // 2, 2 * rows),
        v(n_tp, fh // 2, 2 * rows),
        v(n_tp, fh, 128),
        v(1, d, dtype=F32),
        v(1, HD, dtype=F32),
        v(1, HD, dtype=F32),
        v(1, tq, dtype=F32),
        v(1, HD, dtype=F32),
        v(1, d, dtype=F32),
        v(2, toks, dtype=jnp.int32),
        v(2, toks, dtype=F32),
        dma((17,)),
        dma((nz, NCH)),
        dma((nz,)),
        dma,
        dma((2,)),
        dma((2, 6)),
        dma((2,)),
        dma((2, 6)),
        dma((2,)),
        dma((2, 6)),
        dma,
        dma,
        dma,
        dma,
        dma,
        dma,
    ]
    return pl.pallas_call(
        functools.partial(kernel, n_ep, n_tp),
        out_shape=(
            pltpu.VMEM((tq, 128), BF16),
            pltpu.VMEM((toks, 128), BF16),
        ),
        in_specs=[hbm] * 17,
        out_specs=(vm, vm),
        scratch_shapes=scratch,
        compiler_params=pltpu.CompilerParams(
            collective_id=0, has_side_effects=True, vmem_limit_bytes=60 * 1024 * 1024
        ),
    )(
        attn_in,
        mix_gain.reshape(1, -1),
        query_weight.T,
        key_weight.T,
        value_weight.T,
        query_gain.reshape(1, -1),
        key_gain.reshape(1, -1),
        log_cache.reshape(1, -1),
        head_gain.reshape(1, -1),
        out_weight,
        moe_in,
        moe_gain.reshape(1, -1),
        routes.T,
        route_weight.T,
        jnp.swapaxes(expert_gate, 1, 2),
        jnp.swapaxes(expert_up, 1, 2),
        expert_down,
    )


def solution(mesh):
    n_ep, n_tp = mesh.shape["ep"], mesh.shape["tp"]
    in_specs = (
        P("ep", None),
        P(),
        P(None, "tp"),
        P(None, "tp"),
        P(None, "tp"),
        P(),
        P(),
        P("ep", "tp"),
        P("tp"),
        P(None, "tp"),
        P("ep", None),
        P(),
        P("ep", None),
        P("ep", None),
        P("ep", None, "tp"),
        P("ep", None, "tp"),
        P("ep", "tp", None),
    )
    out_specs = (P("ep", "tp"), P("ep", "tp"))
    return jax.shard_map(
        functools.partial(body, n_ep, n_tp),
        mesh=mesh,
        in_specs=in_specs,
        out_specs=out_specs,
        check_vma=False,
    )
```

```python
import functools

import jax
import jax.numpy as jnp
from jax import lax
from jax.experimental import pallas as pl
from jax.experimental.pallas import tpu as pltpu
from jax.sharding import PartitionSpec as P

HD = 64
EPS = 1e-06
GR = 8
KR = HD + GR
BR = KR + HD
SIDE = 4
SLOT = 16
NCH = 4
NH = NCH // 2
DISPATCH_AFTER = 0
MESH = pl.DeviceIdType.MESH
F32 = jnp.float32
BF16 = jnp.bfloat16


def dot(a, b, dims=((1,), (0,))):
    return lax.dot_general(a, b, (dims, ((), ())), preferred_element_type=F32)


def iota(shape, dim):
    return lax.broadcasted_iota(jnp.int32, shape, dim)


def norm_rows(x, gain):
    return x * lax.rsqrt(jnp.mean(x * x, axis=-1, keepdims=True) + EPS) * gain


def norm_cols(x, gain):
    return x * lax.rsqrt(jnp.mean(x * x, axis=0, keepdims=True) + EPS) * gain


def to_col(row):
    n = row.shape[1]
    eye = iota((n, n), 0) == iota((n, n), 1)
    return jnp.sum(jnp.where(eye, row, 0.0), axis=1, keepdims=True)


def local(src, dst, sem):
    return pltpu.make_async_copy(src, dst, sem)


def send(src, dst, ssem, rsem, ep, tp):
    return pltpu.make_async_remote_copy(
        src_ref=src,
        dst_ref=dst,
        send_sem=ssem,
        recv_sem=rsem,
        device_id=(ep, tp),
        device_id_type=MESH,
    )


class Torus:
    def __init__(self, colour, ep, tp):
        y, x = lax.div(tp, SIDE), lax.rem(tp, SIDE)
        self.ep, self.tp, self.colour = ep, tp, colour
        self.a, self.b = (y, x) if colour == 0 else (x, y)

    def at(self, a, b):
        a, b = lax.rem(a + SIDE, SIDE), lax.rem(b + SIDE, SIDE)
        return a * SIDE + b if self.colour == 0 else b * SIDE + a


class Gather:
    def __init__(self, torus, buf, ssem, rsem):
        self.t, self.buf, self.ss, self.rs = torus, buf, ssem, rsem
        a, b = torus.a, torus.b
        self.am, self.ap = (lax.rem(a + k, SIDE) for k in (3, 1))
        self.bm, self.bp, self.bo = (lax.rem(b + k, SIDE) for k in (3, 1, 2))
        self.across_b = torus.at(a, b + 2)
        self.right_b, self.left_b = torus.at(a, b + 1), torus.at(a, b - 1)
        self.right_a, self.left_a = torus.at(a + 1, b), torus.at(a - 1, b)

    def put(self, block):
        self.buf[SIDE * self.t.a + self.t.b] = block

    def go(self, a, b, to, k):
        src = self.buf.at[SIDE * a + b]
        send(src, src, self.ss, self.rs.at[k], self.t.ep, to).start()

    def whole(self, n, k):
        d = self.buf.at[pl.ds(0, n)]
        return send(d, d, self.ss, self.rs.at[k], self.t.ep, self.t.tp)

    def got(self, k, n):
        self.whole(n, k).wait_recv()

    def stage(self, k):
        a, b = self.t.a, self.t.b
        if k == 0:
            self.go(a, b, self.across_b, 0)
            self.go(a, b, self.right_b, 0)
            self.go(a, b, self.left_b, 0)
        elif k == 1:
            self.got(0, 3)
        elif k == 2:
            self.got(1, 2)
            self.go(self.am, b, self.right_a, 3)
            self.got(2, 6)
            self.go(self.am, self.bm, self.right_a, 3)
            self.go(self.ap, self.bp, self.left_a, 3)
            self.go(self.ap, self.bo, self.left_a, 3)
        else:
            self.got(3, 4)
            self.whole(SIDE * SIDE - 1, 3).wait_send()

    def second(self, k):
        a, b = self.t.a, self.t.b
        if k == 0:
            self.go(a, b, self.right_a, 1)
            self.go(a, b, self.left_a, 1)
        elif k == 1:
            for j in (self.bm, self.bp, self.bo):
                self.go(a, j, self.right_a, 2)
                self.go(a, j, self.left_a, 2)


def step_all(gathers, k):
    for m in gathers:
        m.stage(k)
    for m in gathers:
        m.second(k)


class Exchange:
    def __init__(self, ep, tp, n, cap, src, dst, ssem, rsem):
        self.ep, self.tp, self.n = ep, tp, n
        self.used = pl.ds(0, cap)
        self.src, self.dst, self.ss, self.rs = src, dst, ssem, rsem

    def start(self):
        self.dst[self.ep] = self.src[self.ep]

        def one(i, _):
            step = lax.select(lax.rem(i, 2) == 1, lax.div(i + 1, 2), self.n - lax.div(i, 2))
            peer = lax.rem(self.ep + step, self.n)
            send(
                self.src.at[peer, self.used],
                self.dst.at[self.ep, self.used],
                self.ss,
                self.rs,
                peer,
                self.tp,
            ).start()
            return 0

        lax.fori_loop(1, self.n, one, 0)

    def arrive(self):
        others = pl.ds(0, self.n - 1)
        d = send(
            self.src.at[others, self.used],
            self.dst.at[others, self.used],
            self.ss,
            self.rs,
            self.ep,
            self.tp,
        )
        d.wait_recv()
        d.wait_send()


def kernel(
    n_ep,
    n_tp,
    x_h,
    mix_gain_h,
    wq_h,
    wk_h,
    wv_h,
    q_gain_h,
    k_gain_h,
    gates_h,
    h_gain_h,
    wo_h,
    mx_h,
    moe_gain_h,
    routes_h,
    rweight_h,
    wg_h,
    wu_h,
    wd_h,
    mixer_out,
    moe_out,
    x,
    nx,
    wqkv,
    wo,
    wot,
    wdt,
    to_dense,
    to_wide,
    mx,
    wgu,
    wd,
    kv,
    qa,
    acc,
    mx_run,
    hg0,
    hg1,
    sendb,
    recvb,
    retb,
    backb,
    onehot,
    g0,
    g1,
    h0,
    h1,
    wdn,
    mix_gain,
    q_gain,
    k_gain,
    gates,
    h_gain,
    moe_gain,
    routes,
    rweight,
    load_sem,
    near_recv,
    far_recv,
    kv_send,
    hg_s,
    hg_r,
    mg_s,
    mg_r,
    mh_s,
    mh_r,
    wd_s,
    wd_r,
    d_s,
    d_r,
    b_s,
    b_r,
):
    ep, tp = lax.axis_index("ep"), lax.axis_index("tp")
    z, core = lax.div(ep, 2), lax.rem(ep, 2)
    nz = n_ep // 2
    ups, dns = nz // 2, nz - 1 - nz // 2
    tq = x.shape[0]
    half_t = tq // 2
    fh = wd.shape[0]
    cap = 2 * g0.shape[1] // n_ep

    barrier = pltpu.get_barrier_semaphore()

    def far_first(i):
        return n_ep // 2 + lax.select(lax.rem(i, 2) == 1, lax.div(i, 2), -lax.div(i, 2))

    def greet_ep(i, _):
        pl.semaphore_signal(
            barrier, inc=1, device_id=(lax.rem(ep + far_first(i), n_ep), tp), device_id_type=MESH
        )
        return 0

    def greet_tp(i, _):
        pl.semaphore_signal(
            barrier, inc=1, device_id=(ep, lax.rem(tp + i, n_tp)), device_id_type=MESH
        )
        return 0

    lax.fori_loop(1, n_ep, greet_ep, 0)
    lax.fori_loop(1, n_tp, greet_tp, 0)

    loads = [
        local(s, d, load_sem.at[i])
        for i, (s, d) in enumerate(
            [
                (mx_h, mx),
                (moe_gain_h, moe_gain),
                (routes_h, routes),
                (x_h, x),
                (mix_gain_h, mix_gain),
                (wq_h, wqkv.at[pl.ds(0, HD)]),
                (wk_h, wqkv.at[pl.ds(HD, HD)]),
                (wv_h, wqkv.at[pl.ds(2 * HD, HD)]),
                (q_gain_h, q_gain),
                (k_gain_h, k_gain),
                (gates_h, gates),
                (wg_h.at[0], wgu.at[pl.ds(0, fh)]),
                (wu_h.at[0], wgu.at[pl.ds(fh, fh)]),
                (wd_h.at[0], wd),
                (wo_h, wo),
                (h_gain_h, h_gain),
                (rweight_h, rweight),
            ]
        )
    ]
    for d in loads:
        d.start()

    toks = mx.shape[0]
    slots = n_ep * SLOT
    for d in loads[0:3]:
        d.wait()
    r_rows = [routes[k : k + 1, :].astype(F32) for k in range(2)]
    experts = iota((n_ep, toks), 0).astype(F32)
    hot = [(experts == r).astype(F32) for r in r_rows]
    before = (iota((toks, toks), 0) < iota((toks, toks), 1)).astype(BF16)
    counts = dot((hot[0] + hot[1]).astype(BF16), before)
    for k in range(2):
        order = jnp.sum(hot[k] * counts, axis=0, keepdims=True)
        slot = (r_rows[k] * SLOT + order).astype(jnp.int32)
        onehot[k] = (iota((slots, toks), 0) == slot).astype(F32).astype(BF16)
    mxf = mx[...].astype(F32)
    mscale = lax.rsqrt(jnp.mean(mxf * mxf, axis=-1, keepdims=True) + EPS)
    cols = pl.ds(pl.multiple_of(tp * 128, 128), 128)
    mslice = (mx[:, cols].astype(F32) * mscale * moe_gain[:, cols]).astype(BF16)
    both = (onehot[0].astype(F32) + onehot[1].astype(F32)).astype(BF16)
    sendb[...] = dot(both, mslice).astype(BF16).reshape(n_ep, SLOT, 128)

    for d in loads[3:5]:
        d.wait()

    def norm_some(i, _):
        rows = pl.ds(pl.multiple_of(i * 64, 64), 64)
        nx[rows, :] = norm_rows(x[rows, :].astype(F32), mix_gain[...]).astype(BF16)
        return 0

    lax.fori_loop(0, tq // 64, norm_some, 0)
    for d in loads[5:11]:
        d.wait()
    qkv = dot(wqkv[...], nx[...], ((1,), (1,)))
    q = norm_cols(qkv[0:HD], to_col(q_gain[...])) * (HD**-0.5)
    k = norm_cols(qkv[HD : 2 * HD], to_col(k_gain[...]))
    qa[0:HD, :] = q.astype(BF16)
    ridx = iota((GR, tq), 0)
    qa[HD:KR, :] = jnp.where(ridx < 3, -1.0, 0.0).astype(BF16)
    g = gates[...]
    ghi = g.astype(BF16).astype(F32)
    gmid = (g - ghi).astype(BF16).astype(F32)
    glo = g - ghi - gmid
    grow = jnp.where(
        ridx == 0,
        ghi,
        jnp.where(ridx == 1, gmid, jnp.where(ridx == 2, glo, jnp.where(ridx == 3, 1.0, 0.0))),
    ).astype(BF16)
    kt, vt = k.astype(BF16), qkv[2 * HD :].astype(BF16)
    piece = tq // NCH
    for c in range(NCH):
        cc = slice(c * piece, (c + 1) * piece)
        kv[ep, c, 0:HD, :] = kt[:, cc]
        kv[ep, c, HD:KR, :] = grow[:, cc]
        kv[ep, c, KR:BR, :] = vt[:, cc]

    def pick(rows_out, rows_in, wide_first):
        wide, dense = (0, 1) if wide_first else (1, 0)
        w, d = iota((rows_out, rows_in), wide), iota((rows_out, rows_in), dense)
        i = lax.rem(w, SLOT)
        hit = jnp.logical_and(lax.div(w, SLOT) * cap + i == d, i < cap)
        return hit.astype(F32).astype(BF16)

    to_dense[...] = pick(2 * g0.shape[1], slots, False)
    to_wide[...] = pick(slots, 2 * g0.shape[1], True)
    loads[14].wait()
    wot[...] = wo[...].astype(F32).T.astype(BF16)
    pl.semaphore_wait(barrier, n_ep - 1 + n_tp - 1)

    dispatch = Exchange(ep, tp, n_ep, cap, sendb, recvb, d_s, d_r)

    def features(t):
        return wd.at[:, pl.ds(pl.multiple_of(t * 128, 128), 128)]

    def give_weights(i, _):
        peer = lax.rem(tp + i, n_tp)
        send(features(peer), wdn.at[tp], wd_s, wd_r, ep, peer).start()
        return 0

    def take_weights():
        others = wdn.at[pl.ds(0, n_tp - 1)]
        w = send(others, others, wd_s, wd_r, ep, tp)
        w.wait_recv()
        w.wait_send()

    def hop(slot, c, to_ep):
        piece_ref, sem = kv.at[slot, c], near_recv.at[lax.div(slot, 2), c]
        return send(piece_ref, piece_ref, kv_send, sem, to_ep, tp)

    def hand(slot, c):
        piece_ref, sem = kv.at[slot, c], far_recv.at[lax.div(slot, 2)]
        return send(piece_ref, piece_ref, kv_send, sem, sib_ep, tp)

    up_ep = lax.rem(z + 1, nz) * 2 + core
    dn_ep = lax.rem(z + nz - 1, nz) * 2 + core
    sib_ep = z * 2 + 1 - core

    def slot_of(step, whose):
        return lax.rem(z + step + nz, nz) * 2 + whose

    for c in range(NCH):
        hop(ep, c, up_ep).start()
        hop(ep, c, dn_ep).start()
        hand(ep, c).start()
        if c == DISPATCH_AFTER:
            dispatch.start()

    def flash(slots_in, diagonal=False):
        top, got = (None, None) if diagonal else (mx_run[...], acc[...])
        halves = [
            [jnp.concatenate([kv[i, h * NH + c] for c in range(NH)], axis=1) for h in range(2)]
            for i in slots_in
        ]
        scores = [[dot(p[0:KR], qa[...], ((0,), (0,))) for p in pair] for pair in halves]
        for pair, s in zip(halves, scores):
            if diagonal:
                s = [
                    jnp.where(
                        iota((half_t, tq), 0) + h * half_t <= iota((half_t, tq), 1), s[h], -1e30
                    )
                    for h in range(2)
                ]
            new = jnp.maximum(
                jnp.max(s[0], axis=0, keepdims=True), jnp.max(s[1], axis=0, keepdims=True)
            )
            if top is not None:
                new = jnp.maximum(top, new)
                got = got * jnp.exp(top - new)
            w = [jnp.exp(p - new).astype(BF16) for p in s]
            o = dot(
                jnp.concatenate([p[HD:] for p in pair], axis=1), jnp.concatenate(w, axis=0)
            )
            got = o if got is None else got + o
            top = new
        acc[...] = got
        mx_run[...] = top

    loads[13].wait()
    lax.fori_loop(1, n_tp, give_weights, 0)
    wdn[tp] = wd[:, pl.ds(pl.multiple_of(tp * 128, 128), 128)]
    flash([ep], diagonal=True)

    def take(one, other):
        @pl.when(jnp.maximum(one, other) < ep)
        def _():
            flash([one, other])

        @pl.when(jnp.logical_and(jnp.minimum(one, other) < ep, jnp.maximum(one, other) >= ep))
        def _():
            flash([jnp.minimum(one, other)])

    def wait_piece(slot, c):
        hop(slot, c, up_ep).wait_recv()

    def wait_block(slot):
        sem = far_recv.at[lax.div(slot, 2)]
        send(kv.at[slot], kv.at[slot], kv_send, sem, sib_ep, tp).wait_recv()

    t0, t1 = Torus(0, ep, tp), Torus(1, ep, tp)
    rows = g0.shape[1]
    mg = [
        Gather(t0, g0, mg_s.at[0], mg_r.at[0]),
        Gather(t1, g1, mg_s.at[1], mg_r.at[1]),
    ]
    mh = [
        Gather(t0, h0, mh_s.at[0], mh_r.at[0]),
        Gather(t1, h1, mh_s.at[1], mh_r.at[1]),
    ]
    tiles = range(SIDE * SIDE)
    places = [list(tiles), [SIDE * (t % SIDE) + t // SIDE for t in tiles]]
    returns = Exchange(ep, tp, n_ep, cap, retb, backb, b_s, b_r)

    def filled(buf):
        used = iota((n_ep, SLOT, 128), 1) < cap
        return jnp.where(used, buf[...].astype(F32), 0.0).astype(BF16).reshape(slots, 128)

    def pack_rows():
        dispatch.arrive()
        packed = dot(
            to_dense[...], filled(recvb)
        ).astype(BF16)
        mg[0].put(packed[:rows])
        mg[1].put(packed[rows:])
        step_all(mg, 0)

    def experts_now():
        for d in loads[11:13]:
            d.wait()
        take_weights()
        wdt[...] = wdn[...].reshape(n_tp * fh, 128).astype(F32).T.astype(BF16)
        step_all(mg, 3)
        wide = jnp.concatenate(
            [
                jnp.concatenate([buf[i] for i in place], axis=1)
                for buf, place in zip((g0, g1), places)
            ],
            axis=0,
        )
        sums = dot(wgu[...], wide, ((1,), (1,)))
        gs, us = sums[:fh], sums[fh:]
        hidden = (gs / (1.0 + jnp.exp(-gs)) * us).astype(BF16)
        mh[0].put(hidden[: fh // 2])
        mh[1].put(hidden[fh // 2 :])
        step_all(mh, 0)

    def give_back():
        step_all(mh, 3)
        tall = jnp.concatenate(
            [
                buf[i] for both in zip(*places) for buf, i in zip((h0, h1), both)
            ],
            axis=0,
        )
        rows_out = dot(wdt[...], tall).astype(BF16)
        retb[...] = (
            dot(to_wide[...], rows_out, ((1,), (1,)))
            .astype(BF16)
            .reshape(n_ep, SLOT, 128)
        )
        returns.start()

    hooks = {
        (1, 3): pack_rows,
        (3, 0): lambda: step_all(mg, 1),
        (4, 2): lambda: step_all(mg, 2),
        (6, 0): experts_now,
        (7, 1): lambda: step_all(mh, 1),
        (8, 1): lambda: step_all(mh, 2),
    }

    def run_hooks(s, part):
        for (at, which), hook in hooks.items():
            if which == part and at <= ups:

                @pl.when(s == at)
                def _():
                    hook()

    def ring(s, _):
        up, dn = slot_of(-s, core), slot_of(s, core)
        for c in range(NCH):
            wait_piece(up, c)

            @pl.when(s < (ups if c < NH else dns))
            def _():
                hop(up, c, up_ep).start()

            hand(up, c).start()

            @pl.when(s <= dns)
            def _():
                wait_piece(dn, c)

                @pl.when(s < (dns if c < NH else ups))
                def _():
                    hop(dn, c, dn_ep).start()

                hand(dn, c).start()

            if c == 1:
                ring_up, ring_dn = slot_of(1 - s, core), slot_of(s - 1, core)
                take(*(lax.select(s >= 2, i, n_ep) for i in (ring_up, ring_dn)))
            elif c == 3:
                far_up, far_dn = slot_of(1 - s, 1 - core), slot_of(s - 1, 1 - core)
                wait_block(far_up)

                @pl.when(s >= 2)
                def _():
                    wait_block(far_dn)

                take(far_up, lax.select(s >= 2, far_dn, n_ep))
            run_hooks(s, c)
        return 0

    lax.fori_loop(1, ups + 1, ring, 0)
    last = slot_of(-ups, 1 - core)
    wait_block(last)
    take(slot_of(-ups, core), last)

    loads[15].wait()
    att = acc[GR:, :] / acc[3:4, :]
    head = norm_cols(att, to_col(h_gain[...])).astype(BF16)
    hg = [
        Gather(t0, hg0, hg_s.at[0], hg_r.at[0]),
        Gather(t1, hg1, hg_s.at[1], hg_r.at[1]),
    ]
    for i, m in enumerate(hg):
        m.put(head[:, i * half_t : (i + 1) * half_t])
    step_all(hg, 0)
    for (at, _), hook in hooks.items():
        if at > ups:
            hook()
    give_back()
    step_all(hg, 1)
    step_all(hg, 2)
    loads[16].wait()
    for i, (m, buf) in enumerate(((hg[0], hg0), (hg[1], hg1))):
        m.stage(3)
        tall = jnp.concatenate([buf[j] for j in places[i]], axis=0)
        o = dot(wot[...], tall)
        mixer_out[i * half_t : (i + 1) * half_t, :] = o.T.astype(BF16)

    returns.arrive()
    back = filled(backb)
    total = None
    for k in range(2):
        got = dot(onehot[k], back, ((0,), (0,))) * to_col(rweight[k : k + 1, :])
        total = got if total is None else total + got
    moe_out[...] = total.astype(BF16)

    most = kv.at[pl.ds(0, n_ep - 1)]
    send(most, most, kv_send, far_recv.at[z], sib_ep, tp).wait_send()


def body(
    n_ep,
    n_tp,
    attn_in,
    mix_gain,
    query_weight,
    key_weight,
    value_weight,
    query_gain,
    key_gain,
    log_cache,
    head_gain,
    out_weight,
    moe_in,
    moe_gain,
    routes,
    route_weight,
    expert_gate,
    expert_up,
    expert_down,
):
    tq, d = attn_in.shape
    toks = moe_in.shape[0]
    fh = expert_down.shape[1]
    cap = 3 * toks * routes.shape[1] // (2 * n_ep)
    rows = n_ep * cap // 2
    vm = pl.BlockSpec(memory_space=pltpu.VMEM)
    hbm = pl.BlockSpec(memory_space=pl.ANY)
    dma = pltpu.SemaphoreType.DMA

    def v(*shape, dtype=BF16):
        return pltpu.VMEM(shape, dtype)

    nz = n_ep // 2
    scratch = [
        v(tq, d),
        v(tq, d),
        v(3 * HD, d),
        v(n_tp * HD, 128),
        v(128, n_tp * HD),
        v(128, n_tp * fh),
        v(2 * rows, n_ep * SLOT),
        v(n_ep * SLOT, 2 * rows),
        v(toks, d),
        v(2 * fh, d),
        v(fh, d),
        v(n_ep, NCH, BR, tq // NCH),
        v(KR, tq),
        v(GR + HD, tq, dtype=F32),
        v(1, tq, dtype=F32),
        v(n_tp, HD, tq // 2),
        v(n_tp, HD, tq // 2),
        v(n_ep, SLOT, 128),
        v(n_ep, SLOT, 128),
        v(n_ep, SLOT, 128),
        v(n_ep, SLOT, 128),
        v(2, n_ep * SLOT, toks),
        v(n_tp, rows, 128),
        v(n_tp, rows, 128),
        v(n_tp, fh // 2, 2 * rows),
        v(n_tp, fh // 2, 2 * rows),
        v(n_tp, fh, 128),
        v(1, d, dtype=F32),
        v(1, HD, dtype=F32),
        v(1, HD, dtype=F32),
        v(1, tq, dtype=F32),
        v(1, HD, dtype=F32),
        v(1, d, dtype=F32),
        v(2, toks, dtype=jnp.int32),
        v(2, toks, dtype=F32),
        dma((17,)),
        dma((nz, NCH)),
        dma((nz,)),
        dma,
        dma((2,)),
        dma((2, 4)),
        dma((2,)),
        dma((2, 4)),
        dma((2,)),
        dma((2, 4)),
        dma,
        dma,
        dma,
        dma,
        dma,
        dma,
    ]
    return pl.pallas_call(
        functools.partial(kernel, n_ep, n_tp),
        out_shape=(
            pltpu.VMEM((tq, 128), BF16),
            pltpu.VMEM((toks, 128), BF16),
        ),
        in_specs=[hbm] * 17,
        out_specs=(vm, vm),
        scratch_shapes=scratch,
        compiler_params=pltpu.CompilerParams(
            collective_id=0, has_side_effects=True, vmem_limit_bytes=60 * 1024 * 1024
        ),
    )(
        attn_in,
        mix_gain.reshape(1, -1),
        query_weight.T,
        key_weight.T,
        value_weight.T,
        query_gain.reshape(1, -1),
        key_gain.reshape(1, -1),
        log_cache.reshape(1, -1),
        head_gain.reshape(1, -1),
        out_weight,
        moe_in,
        moe_gain.reshape(1, -1),
        routes.T,
        route_weight.T,
        jnp.swapaxes(expert_gate, 1, 2),
        jnp.swapaxes(expert_up, 1, 2),
        expert_down,
    )


def solution(mesh):
    n_ep, n_tp = mesh.shape["ep"], mesh.shape["tp"]
    in_specs = (
        P("ep", None),
        P(),
        P(None, "tp"),
        P(None, "tp"),
        P(None, "tp"),
        P(),
        P(),
        P("ep", "tp"),
        P("tp"),
        P(None, "tp"),
        P("ep", None),
        P(),
        P("ep", None),
        P("ep", None),
        P("ep", None, "tp"),
        P("ep", None, "tp"),
        P("ep", "tp", None),
    )
    out_specs = (P("ep", "tp"), P("ep", "tp"))
    return jax.shard_map(
        functools.partial(body, n_ep, n_tp),
        mesh=mesh,
        in_specs=in_specs,
        out_specs=out_specs,
        check_vma=False,
    )
```

```python
import functools

import jax
import jax.numpy as jnp
from jax import lax
from jax.experimental import pallas as pl
from jax.experimental.pallas import tpu as pltpu
from jax.sharding import PartitionSpec as P

HD = 64
EPS = 1e-06
GR = 8
KR = HD + GR
BR = KR + HD
SIDE = 4
SLOT = 16
NCH = 4
NH = NCH // 2
DISPATCH_AFTER = 0
MESH = pl.DeviceIdType.MESH
F32 = jnp.float32
BF16 = jnp.bfloat16


def dot(a, b, dims=((1,), (0,))):
    return lax.dot_general(a, b, (dims, ((), ())), preferred_element_type=F32)


def iota(shape, dim):
    return lax.broadcasted_iota(jnp.int32, shape, dim)


def norm_rows(x, gain):
    return x * lax.rsqrt(jnp.mean(x * x, axis=-1, keepdims=True) + EPS) * gain


def norm_cols(x, gain):
    return x * lax.rsqrt(jnp.mean(x * x, axis=0, keepdims=True) + EPS) * gain


def to_col(row):
    n = row.shape[1]
    eye = iota((n, n), 0) == iota((n, n), 1)
    return jnp.sum(jnp.where(eye, row, 0.0), axis=1, keepdims=True)


def local(src, dst, sem):
    return pltpu.make_async_copy(src, dst, sem)


def send(src, dst, ssem, rsem, ep, tp):
    return pltpu.make_async_remote_copy(
        src_ref=src,
        dst_ref=dst,
        send_sem=ssem,
        recv_sem=rsem,
        device_id=(ep, tp),
        device_id_type=MESH,
    )


class Torus:
    def __init__(self, colour, ep, tp):
        y, x = lax.div(tp, SIDE), lax.rem(tp, SIDE)
        self.ep, self.tp, self.colour = ep, tp, colour
        self.a, self.b = (y, x) if colour == 0 else (x, y)

    def at(self, a, b):
        a, b = lax.rem(a + SIDE, SIDE), lax.rem(b + SIDE, SIDE)
        return a * SIDE + b if self.colour == 0 else b * SIDE + a


class Gather:
    def __init__(self, torus, buf, ssem, rsem):
        self.t, self.buf, self.ss, self.rs = torus, buf, ssem, rsem
        a, b = torus.a, torus.b
        self.am, self.ap = (lax.rem(a + k, SIDE) for k in (3, 1))
        self.bm, self.bp, self.bo = (lax.rem(b + k, SIDE) for k in (3, 1, 2))
        self.across_b = torus.at(a, b + 2)
        self.right_b, self.left_b = torus.at(a, b + 1), torus.at(a, b - 1)
        self.right_a, self.left_a = torus.at(a + 1, b), torus.at(a - 1, b)

    def put(self, block):
        self.buf[SIDE * self.t.a + self.t.b] = block

    def go(self, a, b, to, k):
        src = self.buf.at[SIDE * a + b]
        send(src, src, self.ss, self.rs.at[k], self.t.ep, to).start()

    def whole(self, n, k):
        d = self.buf.at[pl.ds(0, n)]
        return send(d, d, self.ss, self.rs.at[k], self.t.ep, self.t.tp)

    def got(self, k, n):
        self.whole(n, k).wait_recv()

    def stage(self, k):
        a, b = self.t.a, self.t.b
        if k == 0:
            self.go(a, b, self.across_b, 0)
            self.go(a, b, self.right_b, 0)
            self.go(a, b, self.left_b, 0)
        elif k == 1:
            self.got(0, 3)
        elif k == 2:
            self.got(1, 2)
            self.go(self.am, b, self.right_a, 3)
            self.got(2, 3)
            self.go(self.am, self.bm, self.right_a, 3)
            self.go(self.ap, self.bp, self.left_a, 3)
            self.go(self.ap, self.bo, self.left_a, 3)
        else:
            self.got(4, 3)
            self.got(3, 4)
            self.whole(SIDE * SIDE - 1, 3).wait_send()

    def second(self, k):
        a, b = self.t.a, self.t.b
        if k == 0:
            self.go(a, b, self.right_a, 1)
            self.go(a, b, self.left_a, 1)
        elif k == 1:
            self.go(a, self.bm, self.right_a, 2)
            self.go(a, self.bp, self.left_a, 2)
            self.go(a, self.bo, self.left_a, 2)
            self.go(a, self.bp, self.right_a, 4)
            self.go(a, self.bo, self.right_a, 4)
            self.go(a, self.bm, self.left_a, 4)


def step_all(gathers, k):
    for m in gathers:
        m.stage(k)
    for m in gathers:
        m.second(k)


class Exchange:
    def __init__(self, ep, tp, n, cap, src, dst, ssem, rsem):
        self.ep, self.tp, self.n = ep, tp, n
        self.used = pl.ds(0, cap)
        self.src, self.dst, self.ss, self.rs = src, dst, ssem, rsem

    def start(self):
        self.dst[self.ep] = self.src[self.ep]

        def one(i, _):
            step = lax.select(lax.rem(i, 2) == 1, lax.div(i + 1, 2), self.n - lax.div(i, 2))
            peer = lax.rem(self.ep + step, self.n)
            send(
                self.src.at[peer, self.used],
                self.dst.at[self.ep, self.used],
                self.ss,
                self.rs,
                peer,
                self.tp,
            ).start()
            return 0

        lax.fori_loop(1, self.n, one, 0)

    def arrive(self):
        others = pl.ds(0, self.n - 1)
        d = send(
            self.src.at[others, self.used],
            self.dst.at[others, self.used],
            self.ss,
            self.rs,
            self.ep,
            self.tp,
        )
        d.wait_recv()
        d.wait_send()


def kernel(
    n_ep,
    n_tp,
    x_h,
    mix_gain_h,
    wq_h,
    wk_h,
    wv_h,
    q_gain_h,
    k_gain_h,
    gates_h,
    h_gain_h,
    wo_h,
    mx_h,
    moe_gain_h,
    routes_h,
    rweight_h,
    wg_h,
    wu_h,
    wd_h,
    mixer_out,
    moe_out,
    x,
    nx,
    wqkv,
    wo,
    wot,
    wdt,
    to_dense,
    to_wide,
    mx,
    wgu,
    wd,
    kv,
    qa,
    acc,
    mx_run,
    hg0,
    hg1,
    sendb,
    recvb,
    retb,
    backb,
    onehot,
    g0,
    g1,
    h0,
    h1,
    wdn,
    mix_gain,
    q_gain,
    k_gain,
    gates,
    h_gain,
    moe_gain,
    routes,
    rweight,
    load_sem,
    near_recv,
    far_recv,
    kv_send,
    hg_s,
    hg_r,
    mg_s,
    mg_r,
    mh_s,
    mh_r,
    wd_s,
    wd_r,
    d_s,
    d_r,
    b_s,
    b_r,
):
    ep, tp = lax.axis_index("ep"), lax.axis_index("tp")
    z, core = lax.div(ep, 2), lax.rem(ep, 2)
    nz = n_ep // 2
    ups, dns = nz // 2, nz - 1 - nz // 2
    tq = x.shape[0]
    half_t = tq // 2
    fh = wd.shape[0]
    cap = 2 * g0.shape[1] // n_ep

    barrier = pltpu.get_barrier_semaphore()

    def far_first(i):
        return n_ep // 2 + lax.select(lax.rem(i, 2) == 1, lax.div(i, 2), -lax.div(i, 2))

    def greet_ep(i, _):
        pl.semaphore_signal(
            barrier, inc=1, device_id=(lax.rem(ep + far_first(i), n_ep), tp), device_id_type=MESH
        )
        return 0

    def greet_tp(i, _):
        pl.semaphore_signal(
            barrier, inc=1, device_id=(ep, lax.rem(tp + i, n_tp)), device_id_type=MESH
        )
        return 0

    lax.fori_loop(1, n_ep, greet_ep, 0)
    lax.fori_loop(1, n_tp, greet_tp, 0)

    loads = [
        local(s, d, load_sem.at[i])
        for i, (s, d) in enumerate(
            [
                (mx_h, mx),
                (moe_gain_h, moe_gain),
                (routes_h, routes),
                (x_h, x),
                (mix_gain_h, mix_gain),
                (wq_h, wqkv.at[pl.ds(0, HD)]),
                (wk_h, wqkv.at[pl.ds(HD, HD)]),
                (wv_h, wqkv.at[pl.ds(2 * HD, HD)]),
                (q_gain_h, q_gain),
                (k_gain_h, k_gain),
                (gates_h, gates),
                (wg_h.at[0], wgu.at[pl.ds(0, fh)]),
                (wu_h.at[0], wgu.at[pl.ds(fh, fh)]),
                (wd_h.at[0], wd),
                (wo_h, wo),
                (h_gain_h, h_gain),
                (rweight_h, rweight),
            ]
        )
    ]
    for d in loads:
        d.start()

    toks = mx.shape[0]
    slots = n_ep * SLOT
    for d in loads[0:3]:
        d.wait()
    r_rows = [routes[k : k + 1, :].astype(F32) for k in range(2)]
    experts = iota((n_ep, toks), 0).astype(F32)
    hot = [(experts == r).astype(F32) for r in r_rows]
    before = (iota((toks, toks), 0) < iota((toks, toks), 1)).astype(BF16)
    counts = dot((hot[0] + hot[1]).astype(BF16), before)
    for k in range(2):
        order = jnp.sum(hot[k] * counts, axis=0, keepdims=True)
        slot = (r_rows[k] * SLOT + order).astype(jnp.int32)
        onehot[k] = (iota((slots, toks), 0) == slot).astype(F32).astype(BF16)
    mxf = mx[...].astype(F32)
    mscale = lax.rsqrt(jnp.mean(mxf * mxf, axis=-1, keepdims=True) + EPS)
    cols = pl.ds(pl.multiple_of(tp * 128, 128), 128)
    mslice = (mx[:, cols].astype(F32) * mscale * moe_gain[:, cols]).astype(BF16)
    both = (onehot[0].astype(F32) + onehot[1].astype(F32)).astype(BF16)
    sendb[...] = dot(both, mslice).astype(BF16).reshape(n_ep, SLOT, 128)

    for d in loads[3:5]:
        d.wait()

    def norm_some(i, _):
        rows = pl.ds(pl.multiple_of(i * 64, 64), 64)
        nx[rows, :] = norm_rows(x[rows, :].astype(F32), mix_gain[...]).astype(BF16)
        return 0

    lax.fori_loop(0, tq // 64, norm_some, 0)
    for d in loads[5:11]:
        d.wait()
    qkv = dot(wqkv[...], nx[...], ((1,), (1,)))
    q = norm_cols(qkv[0:HD], to_col(q_gain[...])) * (HD**-0.5)
    k = norm_cols(qkv[HD : 2 * HD], to_col(k_gain[...]))
    qa[0:HD, :] = q.astype(BF16)
    ridx = iota((GR, tq), 0)
    qa[HD:KR, :] = jnp.where(ridx < 3, -1.0, 0.0).astype(BF16)
    g = gates[...]
    ghi = g.astype(BF16).astype(F32)
    gmid = (g - ghi).astype(BF16).astype(F32)
    glo = g - ghi - gmid
    grow = jnp.where(
        ridx == 0,
        ghi,
        jnp.where(ridx == 1, gmid, jnp.where(ridx == 2, glo, jnp.where(ridx == 3, 1.0, 0.0))),
    ).astype(BF16)
    kt, vt = k.astype(BF16), qkv[2 * HD :].astype(BF16)
    piece = tq // NCH
    for c in range(NCH):
        cc = slice(c * piece, (c + 1) * piece)
        kv[ep, c, 0:HD, :] = kt[:, cc]
        kv[ep, c, HD:KR, :] = grow[:, cc]
        kv[ep, c, KR:BR, :] = vt[:, cc]

    def pick(rows_out, rows_in, wide_first):
        wide, dense = (0, 1) if wide_first else (1, 0)
        w, d = iota((rows_out, rows_in), wide), iota((rows_out, rows_in), dense)
        i = lax.rem(w, SLOT)
        hit = jnp.logical_and(lax.div(w, SLOT) * cap + i == d, i < cap)
        return hit.astype(F32).astype(BF16)

    to_dense[...] = pick(2 * g0.shape[1], slots, False)
    to_wide[...] = pick(slots, 2 * g0.shape[1], True)
    loads[14].wait()
    wot[...] = wo[...].astype(F32).T.astype(BF16)
    pl.semaphore_wait(barrier, n_ep - 1 + n_tp - 1)

    dispatch = Exchange(ep, tp, n_ep, cap, sendb, recvb, d_s, d_r)

    def features(t):
        return wd.at[:, pl.ds(pl.multiple_of(t * 128, 128), 128)]

    def give_weights(i, _):
        peer = lax.rem(tp + i, n_tp)
        send(features(peer), wdn.at[tp], wd_s, wd_r, ep, peer).start()
        return 0

    def take_weights():
        others = wdn.at[pl.ds(0, n_tp - 1)]
        w = send(others, others, wd_s, wd_r, ep, tp)
        w.wait_recv()
        w.wait_send()

    def hop(slot, c, to_ep):
        piece_ref, sem = kv.at[slot, c], near_recv.at[lax.div(slot, 2), c]
        return send(piece_ref, piece_ref, kv_send, sem, to_ep, tp)

    def hand(slot, c):
        piece_ref, sem = kv.at[slot, c], far_recv.at[lax.div(slot, 2)]
        return send(piece_ref, piece_ref, kv_send, sem, sib_ep, tp)

    up_ep = lax.rem(z + 1, nz) * 2 + core
    dn_ep = lax.rem(z + nz - 1, nz) * 2 + core
    sib_ep = z * 2 + 1 - core

    def slot_of(step, whose):
        return lax.rem(z + step + nz, nz) * 2 + whose

    for c in range(NCH):
        hop(ep, c, up_ep).start()
        hop(ep, c, dn_ep).start()
        hand(ep, c).start()
        if c == DISPATCH_AFTER:
            dispatch.start()

    def flash(slots_in, diagonal=False):
        top, got = (None, None) if diagonal else (mx_run[...], acc[...])
        halves = [
            [jnp.concatenate([kv[i, h * NH + c] for c in range(NH)], axis=1) for h in range(2)]
            for i in slots_in
        ]
        scores = [[dot(p[0:KR], qa[...], ((0,), (0,))) for p in pair] for pair in halves]
        for pair, s in zip(halves, scores):
            if diagonal:
                s = [
                    jnp.where(
                        iota((half_t, tq), 0) + h * half_t <= iota((half_t, tq), 1), s[h], -1e30
                    )
                    for h in range(2)
                ]
            new = jnp.maximum(
                jnp.max(s[0], axis=0, keepdims=True), jnp.max(s[1], axis=0, keepdims=True)
            )
            if top is not None:
                new = jnp.maximum(top, new)
                got = got * jnp.exp(top - new)
            w = [jnp.exp(p - new).astype(BF16) for p in s]
            o = dot(
                jnp.concatenate([p[HD:] for p in pair], axis=1), jnp.concatenate(w, axis=0)
            )
            got = o if got is None else got + o
            top = new
        acc[...] = got
        mx_run[...] = top

    loads[13].wait()
    lax.fori_loop(1, n_tp, give_weights, 0)
    wdn[tp] = wd[:, pl.ds(pl.multiple_of(tp * 128, 128), 128)]
    flash([ep], diagonal=True)

    def take(one, other):
        @pl.when(jnp.maximum(one, other) < ep)
        def _():
            flash([one, other])

        @pl.when(jnp.logical_and(jnp.minimum(one, other) < ep, jnp.maximum(one, other) >= ep))
        def _():
            flash([jnp.minimum(one, other)])

    def wait_piece(slot, c):
        hop(slot, c, up_ep).wait_recv()

    def wait_block(slot):
        sem = far_recv.at[lax.div(slot, 2)]
        send(kv.at[slot], kv.at[slot], kv_send, sem, sib_ep, tp).wait_recv()

    t0, t1 = Torus(0, ep, tp), Torus(1, ep, tp)
    rows = g0.shape[1]
    mg = [
        Gather(t0, g0, mg_s.at[0], mg_r.at[0]),
        Gather(t1, g1, mg_s.at[1], mg_r.at[1]),
    ]
    mh = [
        Gather(t0, h0, mh_s.at[0], mh_r.at[0]),
        Gather(t1, h1, mh_s.at[1], mh_r.at[1]),
    ]
    tiles = range(SIDE * SIDE)
    places = [list(tiles), [SIDE * (t % SIDE) + t // SIDE for t in tiles]]
    returns = Exchange(ep, tp, n_ep, cap, retb, backb, b_s, b_r)

    def filled(buf):
        used = iota((n_ep, SLOT, 128), 1) < cap
        return jnp.where(used, buf[...].astype(F32), 0.0).astype(BF16).reshape(slots, 128)

    def pack_rows():
        dispatch.arrive()
        packed = dot(
            to_dense[...], filled(recvb)
        ).astype(BF16)
        mg[0].put(packed[:rows])
        mg[1].put(packed[rows:])
        step_all(mg, 0)

    def experts_now():
        for d in loads[11:13]:
            d.wait()
        take_weights()
        wdt[...] = wdn[...].reshape(n_tp * fh, 128).astype(F32).T.astype(BF16)
        step_all(mg, 3)
        wide = jnp.concatenate(
            [
                jnp.concatenate([buf[i] for i in place], axis=1)
                for buf, place in zip((g0, g1), places)
            ],
            axis=0,
        )
        sums = dot(wgu[...], wide, ((1,), (1,)))
        gs, us = sums[:fh], sums[fh:]
        hidden = (gs / (1.0 + jnp.exp(-gs)) * us).astype(BF16)
        mh[0].put(hidden[: fh // 2])
        mh[1].put(hidden[fh // 2 :])
        step_all(mh, 0)

    def give_back():
        step_all(mh, 3)
        tall = jnp.concatenate(
            [
                buf[i] for both in zip(*places) for buf, i in zip((h0, h1), both)
            ],
            axis=0,
        )
        rows_out = dot(wdt[...], tall).astype(BF16)
        retb[...] = (
            dot(to_wide[...], rows_out, ((1,), (1,)))
            .astype(BF16)
            .reshape(n_ep, SLOT, 128)
        )
        returns.start()

    hooks = {
        (1, 3): pack_rows,
        (3, 0): lambda: step_all(mg, 1),
        (4, 2): lambda: step_all(mg, 2),
        (6, 0): experts_now,
        (7, 1): lambda: step_all(mh, 1),
        (8, 1): lambda: step_all(mh, 2),
    }

    def run_hooks(s, part):
        for (at, which), hook in hooks.items():
            if which == part and at <= ups:

                @pl.when(s == at)
                def _():
                    hook()

    def ring(s, _):
        up, dn = slot_of(-s, core), slot_of(s, core)
        for c in range(NCH):
            wait_piece(up, c)

            @pl.when(s < (ups if c < NH else dns))
            def _():
                hop(up, c, up_ep).start()

            hand(up, c).start()

            @pl.when(s <= dns)
            def _():
                wait_piece(dn, c)

                @pl.when(s < (dns if c < NH else ups))
                def _():
                    hop(dn, c, dn_ep).start()

                hand(dn, c).start()

            if c == 1:
                ring_up, ring_dn = slot_of(1 - s, core), slot_of(s - 1, core)
                take(*(lax.select(s >= 2, i, n_ep) for i in (ring_up, ring_dn)))
            elif c == 3:
                far_up, far_dn = slot_of(1 - s, 1 - core), slot_of(s - 1, 1 - core)
                wait_block(far_up)

                @pl.when(s >= 2)
                def _():
                    wait_block(far_dn)

                take(far_up, lax.select(s >= 2, far_dn, n_ep))
            run_hooks(s, c)
        return 0

    lax.fori_loop(1, ups + 1, ring, 0)
    last = slot_of(-ups, 1 - core)
    wait_block(last)
    take(slot_of(-ups, core), last)

    loads[15].wait()
    att = acc[GR:, :] / acc[3:4, :]
    head = norm_cols(att, to_col(h_gain[...])).astype(BF16)
    hg = [
        Gather(t0, hg0, hg_s.at[0], hg_r.at[0]),
        Gather(t1, hg1, hg_s.at[1], hg_r.at[1]),
    ]
    for i, m in enumerate(hg):
        m.put(head[:, i * half_t : (i + 1) * half_t])
    step_all(hg, 0)
    for (at, _), hook in hooks.items():
        if at > ups:
            hook()
    give_back()
    step_all(hg, 1)
    step_all(hg, 2)
    loads[16].wait()
    for i, (m, buf) in enumerate(((hg[0], hg0), (hg[1], hg1))):
        m.stage(3)
        tall = jnp.concatenate([buf[j] for j in places[i]], axis=0)
        o = dot(wot[...], tall)
        mixer_out[i * half_t : (i + 1) * half_t, :] = o.T.astype(BF16)

    returns.arrive()
    back = filled(backb)
    total = None
    for k in range(2):
        got = dot(onehot[k], back, ((0,), (0,))) * to_col(rweight[k : k + 1, :])
        total = got if total is None else total + got
    moe_out[...] = total.astype(BF16)

    most = kv.at[pl.ds(0, n_ep - 1)]
    send(most, most, kv_send, far_recv.at[z], sib_ep, tp).wait_send()


def body(
    n_ep,
    n_tp,
    attn_in,
    mix_gain,
    query_weight,
    key_weight,
    value_weight,
    query_gain,
    key_gain,
    log_cache,
    head_gain,
    out_weight,
    moe_in,
    moe_gain,
    routes,
    route_weight,
    expert_gate,
    expert_up,
    expert_down,
):
    tq, d = attn_in.shape
    toks = moe_in.shape[0]
    fh = expert_down.shape[1]
    cap = 3 * toks * routes.shape[1] // (2 * n_ep)
    rows = n_ep * cap // 2
    vm = pl.BlockSpec(memory_space=pltpu.VMEM)
    hbm = pl.BlockSpec(memory_space=pl.ANY)
    dma = pltpu.SemaphoreType.DMA

    def v(*shape, dtype=BF16):
        return pltpu.VMEM(shape, dtype)

    nz = n_ep // 2
    scratch = [
        v(tq, d),
        v(tq, d),
        v(3 * HD, d),
        v(n_tp * HD, 128),
        v(128, n_tp * HD),
        v(128, n_tp * fh),
        v(2 * rows, n_ep * SLOT),
        v(n_ep * SLOT, 2 * rows),
        v(toks, d),
        v(2 * fh, d),
        v(fh, d),
        v(n_ep, NCH, BR, tq // NCH),
        v(KR, tq),
        v(GR + HD, tq, dtype=F32),
        v(1, tq, dtype=F32),
        v(n_tp, HD, tq // 2),
        v(n_tp, HD, tq // 2),
        v(n_ep, SLOT, 128),
        v(n_ep, SLOT, 128),
        v(n_ep, SLOT, 128),
        v(n_ep, SLOT, 128),
        v(2, n_ep * SLOT, toks),
        v(n_tp, rows, 128),
        v(n_tp, rows, 128),
        v(n_tp, fh // 2, 2 * rows),
        v(n_tp, fh // 2, 2 * rows),
        v(n_tp, fh, 128),
        v(1, d, dtype=F32),
        v(1, HD, dtype=F32),
        v(1, HD, dtype=F32),
        v(1, tq, dtype=F32),
        v(1, HD, dtype=F32),
        v(1, d, dtype=F32),
        v(2, toks, dtype=jnp.int32),
        v(2, toks, dtype=F32),
        dma((17,)),
        dma((nz, NCH)),
        dma((nz,)),
        dma,
        dma((2,)),
        dma((2, 5)),
        dma((2,)),
        dma((2, 5)),
        dma((2,)),
        dma((2, 5)),
        dma,
        dma,
        dma,
        dma,
        dma,
        dma,
    ]
    return pl.pallas_call(
        functools.partial(kernel, n_ep, n_tp),
        out_shape=(
            pltpu.VMEM((tq, 128), BF16),
            pltpu.VMEM((toks, 128), BF16),
        ),
        in_specs=[hbm] * 17,
        out_specs=(vm, vm),
        scratch_shapes=scratch,
        compiler_params=pltpu.CompilerParams(
            collective_id=0, has_side_effects=True, vmem_limit_bytes=60 * 1024 * 1024
        ),
    )(
        attn_in,
        mix_gain.reshape(1, -1),
        query_weight.T,
        key_weight.T,
        value_weight.T,
        query_gain.reshape(1, -1),
        key_gain.reshape(1, -1),
        log_cache.reshape(1, -1),
        head_gain.reshape(1, -1),
        out_weight,
        moe_in,
        moe_gain.reshape(1, -1),
        routes.T,
        route_weight.T,
        jnp.swapaxes(expert_gate, 1, 2),
        jnp.swapaxes(expert_up, 1, 2),
        expert_down,
    )


def solution(mesh):
    n_ep, n_tp = mesh.shape["ep"], mesh.shape["tp"]
    in_specs = (
        P("ep", None),
        P(),
        P(None, "tp"),
        P(None, "tp"),
        P(None, "tp"),
        P(),
        P(),
        P("ep", "tp"),
        P("tp"),
        P(None, "tp"),
        P("ep", None),
        P(),
        P("ep", None),
        P("ep", None),
        P("ep", None, "tp"),
        P("ep", None, "tp"),
        P("ep", "tp", None),
    )
    out_specs = (P("ep", "tp"), P("ep", "tp"))
    return jax.shard_map(
        functools.partial(body, n_ep, n_tp),
        mesh=mesh,
        in_specs=in_specs,
        out_specs=out_specs,
        check_vma=False,
    )
```

```python
import functools

import jax
import jax.numpy as jnp
from jax import lax
from jax.experimental import pallas as pl
from jax.experimental.pallas import tpu as pltpu
from jax.sharding import PartitionSpec as P

HD = 64
EPS = 1e-06
GR = 8
KR = HD + GR
BR = KR + HD
SIDE = 4
SLOT = 16
NCH = 4
NH = NCH // 2
DISPATCH_AFTER = 0
MESH = pl.DeviceIdType.MESH
F32 = jnp.float32
BF16 = jnp.bfloat16


def dot(a, b, dims=((1,), (0,))):
    return lax.dot_general(a, b, (dims, ((), ())), preferred_element_type=F32)


def iota(shape, dim):
    return lax.broadcasted_iota(jnp.int32, shape, dim)


def norm_rows(x, gain):
    return x * lax.rsqrt(jnp.mean(x * x, axis=-1, keepdims=True) + EPS) * gain


def norm_cols(x, gain):
    return x * lax.rsqrt(jnp.mean(x * x, axis=0, keepdims=True) + EPS) * gain


def to_col(row):
    n = row.shape[1]
    eye = iota((n, n), 0) == iota((n, n), 1)
    return jnp.sum(jnp.where(eye, row, 0.0), axis=1, keepdims=True)


def local(src, dst, sem):
    return pltpu.make_async_copy(src, dst, sem)


def send(src, dst, ssem, rsem, ep, tp):
    return pltpu.make_async_remote_copy(
        src_ref=src,
        dst_ref=dst,
        send_sem=ssem,
        recv_sem=rsem,
        device_id=(ep, tp),
        device_id_type=MESH,
    )


class Torus:
    def __init__(self, colour, ep, tp):
        y, x = lax.div(tp, SIDE), lax.rem(tp, SIDE)
        self.ep, self.tp, self.colour = ep, tp, colour
        self.a, self.b = (y, x) if colour == 0 else (x, y)

    def at(self, a, b):
        a, b = lax.rem(a + SIDE, SIDE), lax.rem(b + SIDE, SIDE)
        return a * SIDE + b if self.colour == 0 else b * SIDE + a


class Gather:
    def __init__(self, torus, buf, ssem, rsem):
        self.t, self.buf, self.ss, self.rs = torus, buf, ssem, rsem
        a, b = torus.a, torus.b
        self.am, self.ap = (lax.rem(a + k, SIDE) for k in (3, 1))
        self.bm, self.bp, self.bo = (lax.rem(b + k, SIDE) for k in (3, 1, 2))
        self.across_b = torus.at(a, b + 2)
        self.right_b, self.left_b = torus.at(a, b + 1), torus.at(a, b - 1)
        self.right_a, self.left_a = torus.at(a + 1, b), torus.at(a - 1, b)

    def put(self, block):
        self.buf[SIDE * self.t.a + self.t.b] = block

    def go(self, a, b, to, k):
        src = self.buf.at[SIDE * a + b]
        send(src, src, self.ss, self.rs.at[k], self.t.ep, to).start()

    def whole(self, n, k):
        d = self.buf.at[pl.ds(0, n)]
        return send(d, d, self.ss, self.rs.at[k], self.t.ep, self.t.tp)

    def got(self, k, n):
        self.whole(n, k).wait_recv()

    def stage(self, k):
        a, b = self.t.a, self.t.b
        if k == 0:
            self.go(a, b, self.across_b, 0)
            self.go(a, b, self.right_b, 0)
            self.go(a, b, self.left_b, 0)
        elif k == 1:
            self.got(0, 3)
        elif k == 2:
            self.got(1, 2)
            self.go(self.am, b, self.right_a, 3)
            self.got(2, 3)
            self.go(self.am, self.bm, self.right_a, 3)
            self.go(self.ap, self.bp, self.left_a, 3)
            self.go(self.ap, self.bo, self.left_a, 3)
        else:
            self.got(4, 3)
            self.got(3, 4)
            self.whole(SIDE * SIDE - 1, 3).wait_send()

    def second(self, k):
        a, b = self.t.a, self.t.b
        if k == 0:
            self.go(a, b, self.right_a, 1)
            self.go(a, b, self.left_a, 1)
        elif k == 1:
            self.go(a, self.bm, self.right_a, 2)
            self.go(a, self.bp, self.left_a, 2)
            self.go(a, self.bo, self.left_a, 2)
            self.go(a, self.bp, self.right_a, 4)
            self.go(a, self.bo, self.right_a, 4)
            self.go(a, self.bm, self.left_a, 4)


def step_all(gathers, k):
    for m in gathers:
        m.stage(k)
    for m in gathers:
        m.second(k)


class Exchange:
    def __init__(self, ep, tp, n, cap, src, dst, ssem, rsem):
        self.ep, self.tp, self.n = ep, tp, n
        self.used = pl.ds(0, cap)
        self.src, self.dst, self.ss, self.rs = src, dst, ssem, rsem

    def start(self):
        self.dst[self.ep] = self.src[self.ep]

        def one(i, _):
            off = lax.div(i, 2)
            step = self.n // 2 + lax.select(lax.rem(i, 2) == 1, off, -off)
            peer = lax.rem(self.ep + step, self.n)
            send(
                self.src.at[peer, self.used],
                self.dst.at[self.ep, self.used],
                self.ss,
                self.rs,
                peer,
                self.tp,
            ).start()
            return 0

        lax.fori_loop(1, self.n, one, 0)

    def arrive(self):
        others = pl.ds(0, self.n - 1)
        d = send(
            self.src.at[others, self.used],
            self.dst.at[others, self.used],
            self.ss,
            self.rs,
            self.ep,
            self.tp,
        )
        d.wait_recv()
        d.wait_send()


def kernel(
    n_ep,
    n_tp,
    x_h,
    mix_gain_h,
    wq_h,
    wk_h,
    wv_h,
    q_gain_h,
    k_gain_h,
    gates_h,
    h_gain_h,
    wo_h,
    mx_h,
    moe_gain_h,
    routes_h,
    rweight_h,
    wg_h,
    wu_h,
    wd_h,
    mixer_out,
    moe_out,
    x,
    nx,
    wqkv,
    wo,
    wot,
    wdt,
    to_dense,
    to_wide,
    mx,
    wgu,
    wd,
    kv,
    qa,
    acc,
    mx_run,
    hg0,
    hg1,
    sendb,
    recvb,
    retb,
    backb,
    onehot,
    g0,
    g1,
    h0,
    h1,
    wdn,
    mix_gain,
    q_gain,
    k_gain,
    gates,
    h_gain,
    moe_gain,
    routes,
    rweight,
    load_sem,
    near_recv,
    far_recv,
    kv_send,
    hg_s,
    hg_r,
    mg_s,
    mg_r,
    mh_s,
    mh_r,
    wd_s,
    wd_r,
    d_s,
    d_r,
    b_s,
    b_r,
):
    ep, tp = lax.axis_index("ep"), lax.axis_index("tp")
    z, core = lax.div(ep, 2), lax.rem(ep, 2)
    nz = n_ep // 2
    ups, dns = nz // 2, nz - 1 - nz // 2
    tq = x.shape[0]
    half_t = tq // 2
    fh = wd.shape[0]
    cap = 2 * g0.shape[1] // n_ep

    barrier = pltpu.get_barrier_semaphore()

    def far_first(i):
        return n_ep // 2 + lax.select(lax.rem(i, 2) == 1, lax.div(i, 2), -lax.div(i, 2))

    def greet_ep(i, _):
        pl.semaphore_signal(
            barrier, inc=1, device_id=(lax.rem(ep + far_first(i), n_ep), tp), device_id_type=MESH
        )
        return 0

    def greet_tp(i, _):
        pl.semaphore_signal(
            barrier, inc=1, device_id=(ep, lax.rem(tp + i, n_tp)), device_id_type=MESH
        )
        return 0

    lax.fori_loop(1, n_ep, greet_ep, 0)
    lax.fori_loop(1, n_tp, greet_tp, 0)

    loads = [
        local(s, d, load_sem.at[i])
        for i, (s, d) in enumerate(
            [
                (mx_h, mx),
                (moe_gain_h, moe_gain),
                (routes_h, routes),
                (x_h, x),
                (mix_gain_h, mix_gain),
                (wq_h, wqkv.at[pl.ds(0, HD)]),
                (wk_h, wqkv.at[pl.ds(HD, HD)]),
                (wv_h, wqkv.at[pl.ds(2 * HD, HD)]),
                (q_gain_h, q_gain),
                (k_gain_h, k_gain),
                (gates_h, gates),
                (wg_h.at[0], wgu.at[pl.ds(0, fh)]),
                (wu_h.at[0], wgu.at[pl.ds(fh, fh)]),
                (wd_h.at[0], wd),
                (wo_h, wo),
                (h_gain_h, h_gain),
                (rweight_h, rweight),
            ]
        )
    ]
    for d in loads:
        d.start()

    toks = mx.shape[0]
    slots = n_ep * SLOT
    for d in loads[0:3]:
        d.wait()
    r_rows = [routes[k : k + 1, :].astype(F32) for k in range(2)]
    experts = iota((n_ep, toks), 0).astype(F32)
    hot = [(experts == r).astype(F32) for r in r_rows]
    before = (iota((toks, toks), 0) < iota((toks, toks), 1)).astype(BF16)
    counts = dot((hot[0] + hot[1]).astype(BF16), before)
    for k in range(2):
        order = jnp.sum(hot[k] * counts, axis=0, keepdims=True)
        slot = (r_rows[k] * SLOT + order).astype(jnp.int32)
        onehot[k] = (iota((slots, toks), 0) == slot).astype(F32).astype(BF16)
    mxf = mx[...].astype(F32)
    mscale = lax.rsqrt(jnp.mean(mxf * mxf, axis=-1, keepdims=True) + EPS)
    cols = pl.ds(pl.multiple_of(tp * 128, 128), 128)
    mslice = (mx[:, cols].astype(F32) * mscale * moe_gain[:, cols]).astype(BF16)
    both = (onehot[0].astype(F32) + onehot[1].astype(F32)).astype(BF16)
    sendb[...] = dot(both, mslice).astype(BF16).reshape(n_ep, SLOT, 128)

    for d in loads[3:5]:
        d.wait()

    def norm_some(i, _):
        rows = pl.ds(pl.multiple_of(i * 64, 64), 64)
        nx[rows, :] = norm_rows(x[rows, :].astype(F32), mix_gain[...]).astype(BF16)
        return 0

    lax.fori_loop(0, tq // 64, norm_some, 0)
    for d in loads[5:11]:
        d.wait()
    qkv = dot(wqkv[...], nx[...], ((1,), (1,)))
    q = norm_cols(qkv[0:HD], to_col(q_gain[...])) * (HD**-0.5)
    k = norm_cols(qkv[HD : 2 * HD], to_col(k_gain[...]))
    qa[0:HD, :] = q.astype(BF16)
    ridx = iota((GR, tq), 0)
    qa[HD:KR, :] = jnp.where(ridx < 3, -1.0, 0.0).astype(BF16)
    g = gates[...]
    ghi = g.astype(BF16).astype(F32)
    gmid = (g - ghi).astype(BF16).astype(F32)
    glo = g - ghi - gmid
    grow = jnp.where(
        ridx == 0,
        ghi,
        jnp.where(ridx == 1, gmid, jnp.where(ridx == 2, glo, jnp.where(ridx == 3, 1.0, 0.0))),
    ).astype(BF16)
    kt, vt = k.astype(BF16), qkv[2 * HD :].astype(BF16)
    piece = tq // NCH
    for c in range(NCH):
        cc = slice(c * piece, (c + 1) * piece)
        kv[ep, c, 0:HD, :] = kt[:, cc]
        kv[ep, c, HD:KR, :] = grow[:, cc]
        kv[ep, c, KR:BR, :] = vt[:, cc]

    def pick(rows_out, rows_in, wide_first):
        wide, dense = (0, 1) if wide_first else (1, 0)
        w, d = iota((rows_out, rows_in), wide), iota((rows_out, rows_in), dense)
        i = lax.rem(w, SLOT)
        hit = jnp.logical_and(lax.div(w, SLOT) * cap + i == d, i < cap)
        return hit.astype(F32).astype(BF16)

    to_dense[...] = pick(2 * g0.shape[1], slots, False)
    to_wide[...] = pick(slots, 2 * g0.shape[1], True)
    loads[14].wait()
    wot[...] = wo[...].astype(F32).T.astype(BF16)
    pl.semaphore_wait(barrier, n_ep - 1 + n_tp - 1)

    dispatch = Exchange(ep, tp, n_ep, cap, sendb, recvb, d_s, d_r)

    def features(t):
        return wd.at[:, pl.ds(pl.multiple_of(t * 128, 128), 128)]

    def give_weights(i, _):
        peer = lax.rem(tp + i, n_tp)
        send(features(peer), wdn.at[tp], wd_s, wd_r, ep, peer).start()
        return 0

    def take_weights():
        others = wdn.at[pl.ds(0, n_tp - 1)]
        w = send(others, others, wd_s, wd_r, ep, tp)
        w.wait_recv()
        w.wait_send()

    def hop(slot, c, to_ep):
        piece_ref, sem = kv.at[slot, c], near_recv.at[lax.div(slot, 2), c]
        return send(piece_ref, piece_ref, kv_send, sem, to_ep, tp)

    def hand(slot, c):
        piece_ref, sem = kv.at[slot, c], far_recv.at[lax.div(slot, 2)]
        return send(piece_ref, piece_ref, kv_send, sem, sib_ep, tp)

    up_ep = lax.rem(z + 1, nz) * 2 + core
    dn_ep = lax.rem(z + nz - 1, nz) * 2 + core
    sib_ep = z * 2 + 1 - core

    def slot_of(step, whose):
        return lax.rem(z + step + nz, nz) * 2 + whose

    for c in range(NCH):
        hop(ep, c, up_ep).start()
        hop(ep, c, dn_ep).start()
        hand(ep, c).start()
        if c == DISPATCH_AFTER:
            dispatch.start()

    def flash(slots_in, diagonal=False):
        top, got = (None, None) if diagonal else (mx_run[...], acc[...])
        halves = [
            [jnp.concatenate([kv[i, h * NH + c] for c in range(NH)], axis=1) for h in range(2)]
            for i in slots_in
        ]
        scores = [[dot(p[0:KR], qa[...], ((0,), (0,))) for p in pair] for pair in halves]
        for pair, s in zip(halves, scores):
            if diagonal:
                s = [
                    jnp.where(
                        iota((half_t, tq), 0) + h * half_t <= iota((half_t, tq), 1), s[h], -1e30
                    )
                    for h in range(2)
                ]
            new = jnp.maximum(
                jnp.max(s[0], axis=0, keepdims=True), jnp.max(s[1], axis=0, keepdims=True)
            )
            if top is not None:
                new = jnp.maximum(top, new)
                got = got * jnp.exp(top - new)
            w = [jnp.exp(p - new).astype(BF16) for p in s]
            o = dot(
                jnp.concatenate([p[HD:] for p in pair], axis=1), jnp.concatenate(w, axis=0)
            )
            got = o if got is None else got + o
            top = new
        acc[...] = got
        mx_run[...] = top

    loads[13].wait()
    lax.fori_loop(1, n_tp, give_weights, 0)
    wdn[tp] = wd[:, pl.ds(pl.multiple_of(tp * 128, 128), 128)]
    flash([ep], diagonal=True)

    def take(one, other):
        @pl.when(jnp.maximum(one, other) < ep)
        def _():
            flash([one, other])

        @pl.when(jnp.logical_and(jnp.minimum(one, other) < ep, jnp.maximum(one, other) >= ep))
        def _():
            flash([jnp.minimum(one, other)])

    def wait_piece(slot, c):
        hop(slot, c, up_ep).wait_recv()

    def wait_block(slot):
        sem = far_recv.at[lax.div(slot, 2)]
        send(kv.at[slot], kv.at[slot], kv_send, sem, sib_ep, tp).wait_recv()

    t0, t1 = Torus(0, ep, tp), Torus(1, ep, tp)
    rows = g0.shape[1]
    mg = [
        Gather(t0, g0, mg_s.at[0], mg_r.at[0]),
        Gather(t1, g1, mg_s.at[1], mg_r.at[1]),
    ]
    mh = [
        Gather(t0, h0, mh_s.at[0], mh_r.at[0]),
        Gather(t1, h1, mh_s.at[1], mh_r.at[1]),
    ]
    tiles = range(SIDE * SIDE)
    places = [list(tiles), [SIDE * (t % SIDE) + t // SIDE for t in tiles]]
    returns = Exchange(ep, tp, n_ep, cap, retb, backb, b_s, b_r)

    def filled(buf):
        used = iota((n_ep, SLOT, 128), 1) < cap
        return jnp.where(used, buf[...].astype(F32), 0.0).astype(BF16).reshape(slots, 128)

    def pack_rows():
        dispatch.arrive()
        packed = dot(
            to_dense[...], filled(recvb)
        ).astype(BF16)
        mg[0].put(packed[:rows])
        mg[1].put(packed[rows:])
        step_all(mg, 0)

    def experts_now():
        for d in loads[11:13]:
            d.wait()
        take_weights()
        wdt[...] = wdn[...].reshape(n_tp * fh, 128).astype(F32).T.astype(BF16)
        step_all(mg, 3)
        wide = jnp.concatenate(
            [
                jnp.concatenate([buf[i] for i in place], axis=1)
                for buf, place in zip((g0, g1), places)
            ],
            axis=0,
        )
        sums = dot(wgu[...], wide, ((1,), (1,)))
        gs, us = sums[:fh], sums[fh:]
        hidden = (gs / (1.0 + jnp.exp(-gs)) * us).astype(BF16)
        mh[0].put(hidden[: fh // 2])
        mh[1].put(hidden[fh // 2 :])
        step_all(mh, 0)

    def give_back():
        step_all(mh, 3)
        tall = jnp.concatenate(
            [
                buf[i] for both in zip(*places) for buf, i in zip((h0, h1), both)
            ],
            axis=0,
        )
        rows_out = dot(wdt[...], tall).astype(BF16)
        retb[...] = (
            dot(to_wide[...], rows_out, ((1,), (1,)))
            .astype(BF16)
            .reshape(n_ep, SLOT, 128)
        )
        returns.start()

    hooks = {
        (1, 3): pack_rows,
        (3, 0): lambda: step_all(mg, 1),
        (4, 2): lambda: step_all(mg, 2),
        (6, 0): experts_now,
        (7, 1): lambda: step_all(mh, 1),
        (8, 1): lambda: step_all(mh, 2),
    }

    def run_hooks(s, part):
        for (at, which), hook in hooks.items():
            if which == part and at <= ups:

                @pl.when(s == at)
                def _():
                    hook()

    def ring(s, _):
        up, dn = slot_of(-s, core), slot_of(s, core)
        for c in range(NCH):
            wait_piece(up, c)

            @pl.when(s < (ups if c < NH else dns))
            def _():
                hop(up, c, up_ep).start()

            hand(up, c).start()

            @pl.when(s <= dns)
            def _():
                wait_piece(dn, c)

                @pl.when(s < (dns if c < NH else ups))
                def _():
                    hop(dn, c, dn_ep).start()

                hand(dn, c).start()

            if c == 1:
                ring_up, ring_dn = slot_of(1 - s, core), slot_of(s - 1, core)
                take(*(lax.select(s >= 2, i, n_ep) for i in (ring_up, ring_dn)))
            elif c == 3:
                far_up, far_dn = slot_of(1 - s, 1 - core), slot_of(s - 1, 1 - core)
                wait_block(far_up)

                @pl.when(s >= 2)
                def _():
                    wait_block(far_dn)

                take(far_up, lax.select(s >= 2, far_dn, n_ep))
            run_hooks(s, c)
        return 0

    lax.fori_loop(1, ups + 1, ring, 0)
    last = slot_of(-ups, 1 - core)
    wait_block(last)
    take(slot_of(-ups, core), last)

    loads[15].wait()
    att = acc[GR:, :] / acc[3:4, :]
    head = norm_cols(att, to_col(h_gain[...])).astype(BF16)
    hg = [
        Gather(t0, hg0, hg_s.at[0], hg_r.at[0]),
        Gather(t1, hg1, hg_s.at[1], hg_r.at[1]),
    ]
    for i, m in enumerate(hg):
        m.put(head[:, i * half_t : (i + 1) * half_t])
    step_all(hg, 0)
    for (at, _), hook in hooks.items():
        if at > ups:
            hook()
    give_back()
    step_all(hg, 1)
    step_all(hg, 2)
    loads[16].wait()
    for i, (m, buf) in enumerate(((hg[0], hg0), (hg[1], hg1))):
        m.stage(3)
        tall = jnp.concatenate([buf[j] for j in places[i]], axis=0)
        o = dot(wot[...], tall)
        mixer_out[i * half_t : (i + 1) * half_t, :] = o.T.astype(BF16)

    returns.arrive()
    back = filled(backb)
    total = None
    for k in range(2):
        got = dot(onehot[k], back, ((0,), (0,))) * to_col(rweight[k : k + 1, :])
        total = got if total is None else total + got
    moe_out[...] = total.astype(BF16)

    most = kv.at[pl.ds(0, n_ep - 1)]
    send(most, most, kv_send, far_recv.at[z], sib_ep, tp).wait_send()


def body(
    n_ep,
    n_tp,
    attn_in,
    mix_gain,
    query_weight,
    key_weight,
    value_weight,
    query_gain,
    key_gain,
    log_cache,
    head_gain,
    out_weight,
    moe_in,
    moe_gain,
    routes,
    route_weight,
    expert_gate,
    expert_up,
    expert_down,
):
    tq, d = attn_in.shape
    toks = moe_in.shape[0]
    fh = expert_down.shape[1]
    cap = 3 * toks * routes.shape[1] // (2 * n_ep)
    rows = n_ep * cap // 2
    vm = pl.BlockSpec(memory_space=pltpu.VMEM)
    hbm = pl.BlockSpec(memory_space=pl.ANY)
    dma = pltpu.SemaphoreType.DMA

    def v(*shape, dtype=BF16):
        return pltpu.VMEM(shape, dtype)

    nz = n_ep // 2
    scratch = [
        v(tq, d),
        v(tq, d),
        v(3 * HD, d),
        v(n_tp * HD, 128),
        v(128, n_tp * HD),
        v(128, n_tp * fh),
        v(2 * rows, n_ep * SLOT),
        v(n_ep * SLOT, 2 * rows),
        v(toks, d),
        v(2 * fh, d),
        v(fh, d),
        v(n_ep, NCH, BR, tq // NCH),
        v(KR, tq),
        v(GR + HD, tq, dtype=F32),
        v(1, tq, dtype=F32),
        v(n_tp, HD, tq // 2),
        v(n_tp, HD, tq // 2),
        v(n_ep, SLOT, 128),
        v(n_ep, SLOT, 128),
        v(n_ep, SLOT, 128),
        v(n_ep, SLOT, 128),
        v(2, n_ep * SLOT, toks),
        v(n_tp, rows, 128),
        v(n_tp, rows, 128),
        v(n_tp, fh // 2, 2 * rows),
        v(n_tp, fh // 2, 2 * rows),
        v(n_tp, fh, 128),
        v(1, d, dtype=F32),
        v(1, HD, dtype=F32),
        v(1, HD, dtype=F32),
        v(1, tq, dtype=F32),
        v(1, HD, dtype=F32),
        v(1, d, dtype=F32),
        v(2, toks, dtype=jnp.int32),
        v(2, toks, dtype=F32),
        dma((17,)),
        dma((nz, NCH)),
        dma((nz,)),
        dma,
        dma((2,)),
        dma((2, 5)),
        dma((2,)),
        dma((2, 5)),
        dma((2,)),
        dma((2, 5)),
        dma,
        dma,
        dma,
        dma,
        dma,
        dma,
    ]
    return pl.pallas_call(
        functools.partial(kernel, n_ep, n_tp),
        out_shape=(
            pltpu.VMEM((tq, 128), BF16),
            pltpu.VMEM((toks, 128), BF16),
        ),
        in_specs=[hbm] * 17,
        out_specs=(vm, vm),
        scratch_shapes=scratch,
        compiler_params=pltpu.CompilerParams(
            collective_id=0, has_side_effects=True, vmem_limit_bytes=60 * 1024 * 1024
        ),
    )(
        attn_in,
        mix_gain.reshape(1, -1),
        query_weight.T,
        key_weight.T,
        value_weight.T,
        query_gain.reshape(1, -1),
        key_gain.reshape(1, -1),
        log_cache.reshape(1, -1),
        head_gain.reshape(1, -1),
        out_weight,
        moe_in,
        moe_gain.reshape(1, -1),
        routes.T,
        route_weight.T,
        jnp.swapaxes(expert_gate, 1, 2),
        jnp.swapaxes(expert_up, 1, 2),
        expert_down,
    )


def solution(mesh):
    n_ep, n_tp = mesh.shape["ep"], mesh.shape["tp"]
    in_specs = (
        P("ep", None),
        P(),
        P(None, "tp"),
        P(None, "tp"),
        P(None, "tp"),
        P(),
        P(),
        P("ep", "tp"),
        P("tp"),
        P(None, "tp"),
        P("ep", None),
        P(),
        P("ep", None),
        P("ep", None),
        P("ep", None, "tp"),
        P("ep", None, "tp"),
        P("ep", "tp", None),
    )
    out_specs = (P("ep", "tp"), P("ep", "tp"))
    return jax.shard_map(
        functools.partial(body, n_ep, n_tp),
        mesh=mesh,
        in_specs=in_specs,
        out_specs=out_specs,
        check_vma=False,
    )
```
